32 devices in a mesh: sp: 8 (over z, y), tp: 4 (over x, core).
Axes of the slice: x: 2, y: 2, z: 4, core: 2. Of those that a mesh axis runs over, the one named last changes fastest.
Arguments:
- tokens: bfloat16 [2560, 2048], P('sp', 'tp'), may hold values from -6 to 6
- pre_gain: float32 [2, 2048], replicated, may hold values from 0.1 to 1.9
- w_value: bfloat16 [2, 2048, 2048], P(None, 'sp', 'tp'), may hold values from -0.125 to 0.125
- w_gate: bfloat16 [2, 2048, 2048], P(None, 'sp', 'tp'), may hold values from -0.125 to 0.125
- taps: float32 [2, 31, 2048], P(None, None, 'tp'), may hold values from -5 to 5
- norm_gain: float32 [2, 2048], P(None, 'tp'), may hold values from 0.1 to 1.9
- norm_shift: float32 [2, 2048], P(None, 'tp'), may hold values from -3 to 3
- w_out: bfloat16 [2, 2048, 2048], P(None, 'tp', 'sp'), may hold values from -2 to 2
- post_gain: float32 [2, 2048], P(None, 'tp'), may hold values from 0.1 to 1.9
Outputs:
- stream: bfloat16 [2560, 2048], P('sp', 'tp')
The draws below stay inside these ranges and needn't reach their ends.
All inputs are finite; a program needn't handle non-finite values.
Results may differ from the reference program's by a relative error of at most 0.015.
Values may be sent and summed in bfloat16 or wider, within the bound.
A program may use at most 64 MiB of HBM per device.

```python
import jax
import jax.numpy as jnp
from jax import lax

D = 2048
CONV_WIDTH = 31
LAYERS = 2
TOKENS = 2560
N_TP = 4


def draw_taps(key, part):
    first, second, third = jax.random.split(jax.random.fold_in(key, 7), 3)
    base = jax.random.truncated_normal(first, -4.0, 4.0, (LAYERS, CONV_WIDTH, D), jnp.float32) * CONV_WIDTH ** (-0.5)
    channel = jnp.exp(jax.random.uniform(second, (LAYERS, 1, D), jnp.float32, -0.7, 0.7))
    levels = jnp.array([0.4, 0.8, 1.6, 3.2], jnp.float32)
    order = jnp.stack([jax.random.permutation(jax.random.fold_in(third, layer), 4) for layer in range(LAYERS)])
    groups = jnp.repeat(levels[order], D // 4, axis=1)
    return base * channel * groups[:, None, :]


def draw_w_out(key, part):
    first, second = jax.random.split(jax.random.fold_in(key, 11), 2)
    base = jax.random.truncated_normal(first, -4.0, 4.0, (LAYERS, D, D), jnp.float32) * D ** (-0.5)
    levels = jnp.array([0.4, 0.8, 1.6, 3.2], jnp.float32)
    order = jnp.stack([jax.random.permutation(jax.random.fold_in(second, layer), 4) for layer in range(LAYERS)])
    groups = jnp.repeat(levels[order], D // 4, axis=1)
    return (base * groups[:, None, :]).astype(jnp.bfloat16)


def shard_levels(own_key, shape, shards, low, largest):
    loudness = 1.0
    for position, parts in shards:
        draws = jax.random.uniform(jax.random.fold_in(jax.random.fold_in(own_key, 6), position), (parts,), jnp.float32, low / len(shards), largest / len(shards))
        loudness = loudness * jnp.repeat(jnp.exp(draws), shape[position] // parts).reshape((-1,) + (1,) * (len(shape) - 1 - position))
    return loudness


def noise(rng, shape, width, most, pieces=(), dtype=jnp.bfloat16):
    values = jax.random.normal(rng, shape, jnp.float32) * width
    if len(pieces) > 0:
        values = shard_levels(rng, shape, pieces, -0.22, 0.18) * values
    return jnp.clip(values, min=-most, max=most).astype(dtype)


def setup_inputs(seed: int = 0) -> dict:
    keys = jax.random.split(jax.random.key(seed), 10)
    tokens = noise(keys[0], (TOKENS, D), 1.0, 6.0, ((0, 8), (1, 4)))
    pre_gain = jnp.clip(1.0 + 0.18 * jax.random.normal(keys[1], (LAYERS, D), jnp.float32), 0.1, 1.9)
    w_value = noise(keys[2], (LAYERS, D, D), D ** -0.5, 0.125, ((1, 8), (2, 4)))
    w_gate = noise(keys[3], (LAYERS, D, D), D ** -0.5, 0.125, ((1, 8), (2, 4)))
    taps = draw_taps(jax.random.fold_in(keys[9], 71), 0)
    norm_gain = jnp.clip(1.0 + 0.18 * jax.random.normal(keys[5], (LAYERS, D), jnp.float32), 0.1, 1.9)
    norm_shift = noise(keys[6], (LAYERS, D), 0.5, 3.0, ((1, 4),), jnp.float32)
    w_out = draw_w_out(jax.random.fold_in(keys[9], 71), 0)
    post_gain = jnp.clip(1.0 + 0.18 * jax.random.normal(keys[8], (LAYERS, D), jnp.float32), 0.1, 1.9)
    return dict(tokens=tokens, pre_gain=pre_gain, w_value=w_value, w_gate=w_gate, taps=taps, norm_gain=norm_gain, norm_shift=norm_shift, w_out=w_out, post_gain=post_gain)


EPSILON = 1e-06
LN_EPSILON = 1e-05

def reference(tokens, pre_gain, w_value, w_gate, taps, norm_gain, norm_shift, w_out, post_gain):
    stream = tokens
    block = D // N_TP
    for layer in range(LAYERS):
        stream_f = stream.astype(jnp.float32)
        normed = (stream_f * lax.rsqrt(lax.optimization_barrier(jnp.mean(stream_f * stream_f, -1, keepdims=True)) + EPSILON) * pre_gain[layer]).astype(jnp.bfloat16)
        value_proj = jnp.dot(normed, w_value[layer], preferred_element_type=jnp.float32)
        gate_proj = jnp.dot(normed, w_gate[layer], preferred_element_type=jnp.float32)
        glu_act = (value_proj * jax.nn.sigmoid(gate_proj)).astype(jnp.bfloat16)
        padded = jnp.pad(glu_act.astype(jnp.float32), ((CONV_WIDTH - 1, 0), (0, 0)))
        conv_out = jnp.zeros((TOKENS, D), jnp.float32)
        for offset in range(CONV_WIDTH):
            conv_out = conv_out + taps[layer, offset] * padded[offset:offset + TOKENS]
        center = lax.optimization_barrier(jnp.sum(conv_out, -1, keepdims=True)) / D
        spread = jnp.maximum(lax.optimization_barrier(jnp.sum(conv_out * conv_out, -1, keepdims=True)) / D - center * center, 0.0)
        activated = jax.nn.silu((conv_out - center) * lax.rsqrt(spread + LN_EPSILON) * norm_gain[layer] + norm_shift[layer]).astype(jnp.bfloat16)
        summed = jnp.zeros((TOKENS, D), jnp.float32)
        for start in range(0, D, block):
            partial_sum = jnp.dot(activated[:, start:start + block], w_out[layer, start:start + block, :], preferred_element_type=jnp.float32).astype(jnp.bfloat16)
            partial_sum = lax.optimization_barrier(partial_sum)
            summed = summed + partial_sum.astype(jnp.float32)
        projected = summed.astype(jnp.bfloat16).astype(jnp.float32)
        scale = lax.rsqrt(lax.optimization_barrier(jnp.mean(projected * projected, -1, keepdims=True)) + EPSILON)
        stream = (stream_f + projected * scale * post_gain[layer]).astype(jnp.bfloat16)
    return stream
```

```python
import jax
import jax.numpy as jnp
from jax import lax
from jax.experimental import pallas as pl
from jax.experimental.pallas import tpu as pltpu
from jax.sharding import PartitionSpec as P

D = 2048
CONV_WIDTH = 31
LAYERS = 2


EPSILON = 1e-06
LN_EPSILON = 1e-05


def passed_along(block, axis, distance):
    devices = range(lax.axis_size(axis))
    route = [(i - distance, i) for i in devices if i - distance in devices]
    return lax.ppermute(block, axis, route)


def local(tokens, pre_gain, w_value, w_gate, taps, norm_gain, norm_shift, w_out, post_gain):
    stream = tokens
    full_value, full_gate = (
        lax.all_gather(w_value, "sp", axis=1, tiled=True),
        lax.all_gather(w_gate, "sp", axis=1, tiled=True),
    )
    full_out = lax.all_gather(w_out, "sp", axis=2, tiled=True)
    for layer in range(LAYERS):
        whole = lax.all_gather(stream, "tp", axis=1, tiled=True)
        whole_f = whole.astype(jnp.float32)
        normed = (
            whole_f
            * lax.rsqrt(jnp.mean(whole_f * whole_f, -1, keepdims=True) + EPSILON)
            * pre_gain[layer]
        ).astype(jnp.bfloat16)
        value_mat = full_value[layer]
        gate_mat = full_gate[layer]
        out_mat = full_out[layer]
        value_proj = jnp.dot(normed, value_mat, preferred_element_type=jnp.float32)
        gate_proj = jnp.dot(normed, gate_mat, preferred_element_type=jnp.float32)
        glu_act = (value_proj * jax.nn.sigmoid(gate_proj)).astype(jnp.bfloat16)
        rows = glu_act.shape[0]
        fringe = passed_along(glu_act[rows - (CONV_WIDTH - 1) :], "sp", 1)
        padded = jnp.concatenate([fringe, glu_act], 0).astype(jnp.float32)
        conv_out = jnp.zeros(glu_act.shape, jnp.float32)
        for offset in range(CONV_WIDTH):
            conv_out = conv_out + taps[layer, offset] * padded[offset : offset + rows]
        row_sum, row_square = lax.psum(
            (jnp.sum(conv_out, -1, keepdims=True), jnp.sum(conv_out * conv_out, -1, keepdims=True)),
            "tp",
        )
        center = row_sum / D
        spread = jnp.maximum(row_square / D - center * center, 0.0)
        activated = jax.nn.silu(
            (conv_out - center) * lax.rsqrt(spread + LN_EPSILON) * norm_gain[layer]
            + norm_shift[layer]
        ).astype(jnp.bfloat16)
        terms = jnp.dot(activated, out_mat, preferred_element_type=jnp.float32)
        summed = lax.psum_scatter(terms.astype(jnp.bfloat16), "tp", scatter_dimension=1, tiled=True)
        projected = summed.astype(jnp.float32)
        out_square = lax.psum(jnp.sum(projected * projected, -1, keepdims=True), "tp")
        scale = lax.rsqrt(out_square / D + EPSILON)
        stream = (stream.astype(jnp.float32) + projected * scale * post_gain[layer]).astype(
            jnp.bfloat16
        )
    return stream


TILE = 64
PACK = 16
HALO = 32


def step(
    x_ref, pre_ref, wv_hbm, wg_hbm, taps_ref, ng_ref, ns_ref, wo_hbm, post_ref, out_ref,
    weight, other, whole, normed, glu, conv, act, part_out, part_in, x_out, x_in, z_out, z_in,
    total, taps, gain, shift, stat, stat_in, local_sem,
    zs, zr, ys, yr, gs, gr, hs, hr, ss, sr, ps, pr, xs, xr, bs, br,
):
    sp, tp = lax.axis_index("sp"), lax.axis_index("tp")
    rows, cols = x_ref.shape
    layers = pre_ref.shape[0]
    nsp, ntp = 8, 4
    z, y = sp // 2, sp % 2
    zh, zl = z // 2, z % 2
    x, c = tp // 2, tp % 2
    plane = [z, zh * 2 + 1 - zl, (1 - zh) * 2 + zl, (1 - zh) * 2 + 1 - zl]
    partner = plane[1] * 2 + y
    beside, facing = (partner, tp), (z * 2 + 1 - y, tp)
    mate, across, diagonal = (sp, x * 2 + 1 - c), (sp, (1 - x) * 2 + c), (sp, (1 - x) * 2 + 1 - c)
    units = 3 * layers
    both, half = 2 * rows, cols // 2
    mine = pl.ds(pl.multiple_of(zl * half, half), half)
    rest = pl.ds(pl.multiple_of((1 - zl) * half, half), half)
    depth = wv_hbm.shape[1]

    def copy(src, dst, send, recv, to):
        return pltpu.make_async_remote_copy(
            src_ref=src, dst_ref=dst, send_sem=send, recv_sem=recv, device_id=to,
            device_id_type=pl.DeviceIdType.MESH,
        )

    def piece(u, slot):
        return weight.at[u, pl.ds(pl.multiple_of(slot * depth, depth), depth)]

    def along(u, k):
        p = piece(u, sp)
        return copy(
            p if k == 2 else other.at[u], p, zs.at[u, k - 1], zr.at[u, k - 1], (plane[k] * 2 + y, tp)
        )

    def sideways(u, k):
        p = piece(u, plane[k] * 2 + y)
        return copy(p, p, ys.at[u, k], yr.at[u, k], facing)

    def own(u):
        for k in (3, 2, 1):
            along(u, k).start()
        sideways(u, 0).start()

    def relay(u, k):
        p = piece(u, plane[k] * 2 + y)
        copy(p, p, zs.at[u, k - 1], zr.at[u, k - 1], beside).wait_recv()
        sideways(u, k).start()

    def arrive(u):
        for k in range(4):
            p = piece(u, plane[k] * 2 + 1 - y)
            copy(p, p, ys.at[u, k], yr.at[u, k], facing).wait_recv()

    here, there = zl * 4, (1 - zl) * 4
    opposite = (1 - x) * 2 + c

    routes = dict(
        across=(here + tp, across),
        beside=(here + tp, beside),
        mate=(here + tp, mate),
        across_mate=(here + opposite, mate),
        beside_across=(there + tp, across),
        beside_mate=(there + tp, mate),
        both_mate=(there + opposite, mate),
        across_beside=(here + opposite, beside),
    )
    upper, lower = pl.ds(0, rows // 2), pl.ds(rows // 2, rows // 2)
    parts = dict(beside_across=upper, across_beside=lower)

    def gather(l, name):
        k = list(routes).index(name)
        t, to = routes[name]
        b = whole.at[l, t, parts[name]] if name in parts else whole.at[l, t]
        return copy(b, b, gs.at[l, k], gr.at[l, k], to)

    def came(l, k, t, part=pl.ds(0, rows)):
        b = whole.at[l, t, part]
        copy(b, b, gs.at[l, k], gr.at[l, k], mate).wait_recv()

    def gather_start(l):
        for name in ("across", "beside", "mate"):
            gather(l, name).start()

    def gather_turn(l):
        came(l, 1, there + tp)
        gather(l, "beside_across").start()
        gather(l, "beside_mate").start()
        came(l, 0, here + opposite)
        gather(l, "across_beside").start()
        gather(l, "across_mate").start()

    def gather_last(l):
        came(l, 4, there + opposite, upper)
        came(l, 7, there + opposite, lower)
        gather(l, "both_mate").start()

    def gather_wait(l):
        pair_tp, pair_opposite = x * 2 + 1 - c, (1 - x) * 2 + 1 - c
        came(l, 2, here + pair_tp)
        came(l, 3, here + pair_opposite)
        came(l, 5, there + pair_tp)
        came(l, 6, there + pair_opposite)

    def norm(l):
        gather_wait(l)
        tiles = rows // TILE

        @pl.loop(0, 2 * tiles)
        def _(i):
            g, r = i // tiles * 4, pl.ds(pl.multiple_of(i % tiles * TILE, TILE), TILE)
            to = pl.ds(pl.multiple_of(i * TILE, TILE), TILE)
            square = jnp.zeros((TILE, 1), jnp.float32)
            for t in range(ntp):
                v = whole[l, g + t, r, :].astype(jnp.float32)
                square = square + jnp.sum(v * v, -1, keepdims=True)
            scale = lax.rsqrt(square / (cols * ntp) + EPSILON)
            for t in range(ntp):
                v = whole[l, g + t, r, :].astype(jnp.float32)
                at = slice(t * cols, (t + 1) * cols)
                normed[to, at] = (v * scale * pre_ref[l : l + 1, at]).astype(jnp.bfloat16)

    tail, head = pl.ds(rows, HALO), pl.ds(0, HALO)

    def near_halo(l):
        return copy(glu.at[l, 0, tail], glu.at[l, y, head], hs.at[l, 0], hr.at[l, y], facing)

    def even_halo(l):
        return copy(glu.at[l, 1, tail], glu.at[l, 1, head], hs.at[l, 1], hr.at[l, 1], facing)

    def odd_halo(l):
        return copy(
            glu.at[l, 1, tail], glu.at[l, 0, head], hs.at[l, 1], hr.at[l, 0], ((z + 2) * 2, tp)
        )

    def halo_send(l, act_on):
        act_on(near_halo(l))
        pl.when(y == 0)(lambda: act_on(even_halo(l)))
        pl.when((y == 1) & (zh == 0))(lambda: act_on(odd_halo(l)))

    def halo_wait(l):
        def got(q):
            b = glu.at[l, q, head]
            copy(b, b, hs.at[l, q], hr.at[l, q], facing).wait_recv()

        pl.when((y == 1) | (zh == 1))(lambda: got(0))
        got(1)

        @pl.when((y == 0) & (zh == 0))
        def _():
            glu[l, 0, :HALO] = jnp.zeros((HALO, half), jnp.bfloat16)

    def project(l):
        n = normed[...]
        value = jnp.dot(n, weight[3 * l], preferred_element_type=jnp.float32)
        gate = jnp.dot(n, weight[3 * l + 1], preferred_element_type=jnp.float32)
        made = (value * jax.nn.sigmoid(gate)).astype(jnp.bfloat16)
        glu[l, 0, HALO:, :] = made[:rows]
        glu[l, 1, HALO:, :] = made[rows:]
        halo_send(l, lambda h: h.start())

    peers = [mate, across, diagonal, beside]
    peers += [(partner, mate[1]), (partner, across[1]), (partner, diagonal[1])]

    def exchange(e):
        return [
            copy(stat.at[e], stat_in.at[e, j], ss.at[e, j], sr.at[e, j], to)
            for j, to in enumerate(peers[: 3 if e % 2 else 7])
        ]

    def exchanged(e):
        sums = stat[e]
        for j, s in enumerate(exchange(e)):
            s.wait_recv()
            sums = sums + stat_in[e, j]
        return sums

    lane = lax.broadcasted_iota(jnp.int32, (PACK, 128), 1)
    groups = TILE // PACK

    def pick(sums, at):
        found = [
            jnp.sum(jnp.where(lane == at * groups + g, sums, 0.0), -1, keepdims=True)
            for g in range(groups)
        ]
        return jnp.concatenate(found, 0)

    def pack(sums, at, column):
        for g in range(groups):
            sums = jnp.where(lane == at * groups + g, column[g * PACK : (g + 1) * PACK], sums)
        return sums

    tiles = rows // TILE

    def convolve(l):
        first = HALO - (CONV_WIDTH - 1)

        def tile(q, i, sums):
            r = pl.multiple_of(i * TILE, TILE)
            one = jnp.zeros((TILE, 128), jnp.float32)
            two = jnp.zeros((TILE, 128), jnp.float32)
            for j in range(half // 128):
                at = slice(j * 128, (j + 1) * 128)
                window = glu[l, q, pl.ds(r, TILE + HALO), at].astype(jnp.float32)
                acc = jnp.zeros((TILE, 128), jnp.float32)
                for s in range(8):
                    w = window if s == 0 else pltpu.roll(window, TILE + HALO - s, 0)
                    for k in range(CONV_WIDTH):
                        if (first + k) % 8 == s:
                            o = first + k - s
                            acc = acc + taps[l, k : k + 1, at] * w[o : o + TILE]
                conv[q, pl.ds(r, TILE), at] = acc
                one = one + acc
                two = two + acc * acc
            n = q * tiles + i
            sums = pack(sums, 2 * n, jnp.sum(one, -1, keepdims=True))
            return pack(sums, 2 * n + 1, jnp.sum(two, -1, keepdims=True))

        inner = tiles - 1
        sums = lax.fori_loop(
            0, 2 * inner, lambda i, s: tile(i // inner, i % inner + 1, s),
            jnp.zeros((PACK, 128), jnp.float32),
        )
        halo_wait(l)
        stat[2 * l] = lax.fori_loop(0, 2, lambda q, s: tile(q, 0, s), sums)
        for s in exchange(2 * l):
            s.start()

    def activate(l):
        sums = exchanged(2 * l)

        @pl.loop(0, 2 * tiles)
        def _(at):
            q, r = at // tiles, pl.ds(pl.multiple_of(at % tiles * TILE, TILE), TILE)
            center = pick(sums, 2 * at) / (cols * ntp)
            spread = jnp.maximum(pick(sums, 2 * at + 1) / (cols * ntp) - center * center, 0.0)
            v = (conv[q, r, :] - center) * lax.rsqrt(spread + LN_EPSILON)
            v = v * gain[l : l + 1, :] + shift[l : l + 1, :]
            act[q, r, :] = (v * jax.nn.sigmoid(v)).astype(jnp.bfloat16)

    each = wo_hbm.shape[2]
    per = cols // each
    quads = dict(D=(1 - zl, 1 - x), A=(zl, 1 - x), B=(1 - zl, x), O=(zl, x))
    names = list(quads)

    def term(l, quad, h, core):
        q, column = quads[quad]
        slot = (column * 2 + core) * per + h
        w = weight[3 * l + 2, pl.ds(pl.multiple_of(slot * depth, depth), depth), :]
        return jnp.dot(act[q], w, preferred_element_type=jnp.float32).astype(jnp.bfloat16)

    def pair(l, quad, h):
        i = names.index(quad) * per + h
        return copy(part_out.at[l, i], part_in.at[l, i], ps.at[l, i], pr.at[l, i], mate)

    def over(l, i):
        return copy(x_out.at[l, i], x_in.at[l, i], xs.at[l, i], xr.at[l, i], across)

    def along_pair(l, i):
        return copy(z_out.at[l, i], z_in.at[l, i], bs.at[l, i], br.at[l, i], beside)

    def give(l, quad, h):
        part_out[l, names.index(quad) * per + h] = term(l, quad, h, 1 - c)
        pair(l, quad, h).start()

    def joined(l, quad, h):
        kept = term(l, quad, h, c).astype(jnp.float32)
        pair(l, quad, h).wait_recv()
        return kept + part_in[l, names.index(quad) * per + h].astype(jnp.float32)

    def pass_x(l, i, v):
        x_out[l, i] = v.astype(jnp.bfloat16)
        over(l, i).start()

    def pass_z(l, i, v):
        z_out[l, i] = v.astype(jnp.bfloat16)
        along_pair(l, i).start()

    def reduce(l, between):
        give(l, "D", 0)
        give(l, "D", 1)
        give(l, "A", 0)
        give(l, "B", 1)
        pass_x(l, 0, joined(l, "D", 0))
        pass_z(l, 0, joined(l, "D", 1))
        give(l, "A", 1)
        give(l, "B", 0)
        pass_x(l, 1, joined(l, "A", 0))
        pass_z(l, 1, joined(l, "B", 1))
        give(l, "O", 0)
        give(l, "O", 1)
        for h in range(per):
            total[:, h * each : (h + 1) * each] = joined(l, "O", h)
        from_beside = joined(l, "A", 1)
        along_pair(l, 0).wait_recv()
        pass_x(l, 2, from_beside + z_in[l, 0].astype(jnp.float32))
        from_across = joined(l, "B", 0)
        over(l, 0).wait_recv()
        pass_z(l, 2, from_across + x_in[l, 0].astype(jnp.float32))
        between()

    def finish(l):
        over(l, 1).wait_recv()
        along_pair(l, 1).wait_recv()
        over(l, 2).wait_recv()
        along_pair(l, 2).wait_recv()

        def tile(i, sums):
            r = pl.ds(pl.multiple_of(i * TILE, TILE), TILE)
            square = jnp.zeros((TILE, 1), jnp.float32)
            for h in range(per):
                at = slice(h * each, (h + 1) * each)
                p = total[r, at] + x_in[l, 1 + h, r, :].astype(jnp.float32)
                p = p + z_in[l, 2 - h, r, :].astype(jnp.float32)
                p = p.astype(jnp.bfloat16).astype(jnp.float32)
                total[r, at] = p
                square = square + jnp.sum(p * p, -1, keepdims=True)
            return pack(sums, i, square)

        e = 2 * l + 1
        stat[e] = lax.fori_loop(0, tiles, tile, jnp.zeros((PACK, 128), jnp.float32))
        for s in exchange(e):
            s.start()
        sums = exchanged(e)

        @pl.loop(0, tiles)
        def _(i):
            r = pl.ds(pl.multiple_of(i * TILE, TILE), TILE)
            scale = lax.rsqrt(pick(sums, i) / (cols * ntp) + EPSILON)
            old = whole[l, here + tp, r, :].astype(jnp.float32)
            new = (old + total[r, :] * scale * post_ref[l : l + 1, :]).astype(jnp.bfloat16)
            if l + 1 < layers:
                whole[l + 1, here + tp, r, :] = new
            else:
                out_ref[r, :] = new

    held = [pltpu.make_async_copy(x_ref, whole.at[0, here + tp], local_sem.at[2 * units])]
    for u in range(units):
        l, kind = divmod(u, 3)
        ref = (wv_hbm, wg_hbm, wo_hbm)[kind]
        for i, (part, to) in enumerate(((mine, piece(u, sp)), (rest, other.at[u]))):
            src = ref.at[l, part] if kind == 2 else ref.at[l, :, part]
            held.append(pltpu.make_async_copy(src, to, local_sem.at[2 * u + i]))
    for h in held:
        h.start()
    for l in range(layers):
        taps[l] = taps_ref[l, :, mine]
        gain[l : l + 1] = ng_ref[l : l + 1, mine]
        shift[l : l + 1] = ns_ref[l : l + 1, mine]
    barrier = pltpu.get_barrier_semaphore()
    for i in range(1, nsp):
        pl.semaphore_signal(
            barrier, inc=1, device_id=(lax.rem(sp + i, nsp), tp),
            device_id_type=pl.DeviceIdType.MESH,
        )
    for i in range(1, ntp):
        for at in (sp, partner):
            pl.semaphore_signal(
                barrier, inc=1, device_id=(at, lax.rem(tp + i, ntp)),
                device_id_type=pl.DeviceIdType.MESH,
            )
    pl.semaphore_wait(barrier, nsp - 1 + 2 * (ntp - 1))
    for h in held:
        h.wait()

    far = range(1, 4)
    gather_start(0)
    own(0)
    own(1)
    gather_turn(0)
    own(2)
    for k in far:
        relay(0, k)
    gather_last(0)
    norm(0)
    for k in far:
        relay(1, k)
    arrive(0)
    arrive(1)
    project(0)
    relay(2, 1)
    convolve(0)
    relay(2, 2)
    relay(2, 3)
    activate(0)
    arrive(2)
    reduce(0, lambda: (own(3), own(4)))
    finish(0)
    gather_start(1)
    own(5)
    for k in far:
        relay(3, k)
    gather_turn(1)
    for k in far:
        relay(4, k)
    gather_last(1)
    norm(1)
    arrive(3)
    arrive(4)
    project(1)
    relay(5, 1)
    convolve(1)
    relay(5, 2)
    relay(5, 3)
    activate(1)
    arrive(5)
    reduce(1, lambda: None)
    finish(1)

    sent = [along(u, k) for u in range(units) for k in far]
    sent += [sideways(u, k) for u in range(units) for k in range(4)]
    for l in range(layers):
        sent += [gather(l, name) for name in routes]
        sent += [*exchange(2 * l), *exchange(2 * l + 1)]
        sent += [over(l, i) for i in range(3)] + [along_pair(l, i) for i in range(3)]
        sent += [pair(l, quad, h) for quad in names for h in range(per)]
        halo_send(l, lambda h: h.wait_send())
    for s in sent:
        s.wait_send()


def kernel_local(*args):
    tokens, pre_gain, w_value, _, _, _, _, w_out, _ = args
    rows, cols = tokens.shape
    layers, depth = w_value.shape[:2]
    each = w_out.shape[2]
    half, units = cols // 2, 3 * layers
    if rows % TILE or 2 * 2 * rows > PACK * 128 or not depth == half == each:
        return local(*args)
    vmem, hbm = pl.BlockSpec(memory_space=pltpu.VMEM), pl.BlockSpec(memory_space=pl.ANY)
    bf16, f32, dma = jnp.bfloat16, jnp.float32, pltpu.SemaphoreType.DMA
    return pl.pallas_call(
        step,
        out_shape=jax.ShapeDtypeStruct((rows, cols), bf16),
        in_specs=[hbm, vmem, hbm, hbm, vmem, vmem, vmem, hbm, vmem],
        out_specs=vmem,
        scratch_shapes=[
            pltpu.VMEM((units, 8 * depth, half), bf16),
            pltpu.VMEM((units, depth, half), bf16),
            pltpu.VMEM((layers, 8, rows, cols), bf16),
            pltpu.VMEM((2 * rows, 4 * cols), bf16),
            pltpu.VMEM((layers, 2, HALO + rows, half), bf16),
            pltpu.VMEM((2, rows, half), f32),
            pltpu.VMEM((2, rows, half), bf16),
            pltpu.VMEM((layers, 8, rows, each), bf16),
            pltpu.VMEM((layers, 8, rows, each), bf16),
            pltpu.VMEM((layers, 3, rows, each), bf16),
            pltpu.VMEM((layers, 3, rows, each), bf16),
            pltpu.VMEM((layers, 3, rows, each), bf16),
            pltpu.VMEM((layers, 3, rows, each), bf16),
            pltpu.VMEM((rows, cols), f32),
            pltpu.VMEM((layers, CONV_WIDTH, half), f32),
            pltpu.VMEM((layers, half), f32),
            pltpu.VMEM((layers, half), f32),
            pltpu.VMEM((2 * layers, PACK, 128), f32),
            pltpu.VMEM((2 * layers, 7, PACK, 128), f32),
            dma((2 * units + 1,)),
            dma((units, 3)), dma((units, 3)),
            dma((units, 4)), dma((units, 4)),
            dma((layers, 8)), dma((layers, 8)),
            dma((layers, 2)), dma((layers, 2)),
            dma((2 * layers, 7)), dma((2 * layers, 7)),
            dma((layers, 8)), dma((layers, 8)),
            dma((layers, 3)), dma((layers, 3)),
            dma((layers, 3)), dma((layers, 3)),
        ],
        compiler_params=pltpu.CompilerParams(
            collective_id=0, has_side_effects=True, vmem_limit_bytes=56 * 1024 * 1024
        ),
    )(*args)


def solution(mesh):
    nsp, ntp = mesh.shape["sp"], mesh.shape["tp"]
    body = kernel_local if nsp == 8 and ntp == 4 else local
    placed = (
        P("sp", "tp"),
        P(),
        P(None, "sp", "tp"),
        P(None, "sp", "tp"),
        P(None, None, "tp"),
        P(None, "tp"),
        P(None, "tp"),
        P(None, "tp", "sp"),
        P(None, "tp"),
    )
    return jax.shard_map(
        body, mesh=mesh, in_specs=placed, out_specs=P("sp", "tp"), check_vma=False
    )
```

```python
import jax
import jax.numpy as jnp
from jax import lax
from jax.experimental import pallas as pl
from jax.experimental.pallas import tpu as pltpu
from jax.sharding import PartitionSpec as P

D = 2048
CONV_WIDTH = 31
LAYERS = 2


EPSILON = 1e-06
LN_EPSILON = 1e-05


def passed_along(block, axis, distance):
    devices = range(lax.axis_size(axis))
    route = [(i - distance, i) for i in devices if i - distance in devices]
    return lax.ppermute(block, axis, route)


def local(tokens, pre_gain, w_value, w_gate, taps, norm_gain, norm_shift, w_out, post_gain):
    stream = tokens
    full_value, full_gate = (
        lax.all_gather(w_value, "sp", axis=1, tiled=True),
        lax.all_gather(w_gate, "sp", axis=1, tiled=True),
    )
    full_out = lax.all_gather(w_out, "sp", axis=2, tiled=True)
    for layer in range(LAYERS):
        whole = lax.all_gather(stream, "tp", axis=1, tiled=True)
        whole_f = whole.astype(jnp.float32)
        normed = (
            whole_f
            * lax.rsqrt(jnp.mean(whole_f * whole_f, -1, keepdims=True) + EPSILON)
            * pre_gain[layer]
        ).astype(jnp.bfloat16)
        value_mat = full_value[layer]
        gate_mat = full_gate[layer]
        out_mat = full_out[layer]
        value_proj = jnp.dot(normed, value_mat, preferred_element_type=jnp.float32)
        gate_proj = jnp.dot(normed, gate_mat, preferred_element_type=jnp.float32)
        glu_act = (value_proj * jax.nn.sigmoid(gate_proj)).astype(jnp.bfloat16)
        rows = glu_act.shape[0]
        fringe = passed_along(glu_act[rows - (CONV_WIDTH - 1) :], "sp", 1)
        padded = jnp.concatenate([fringe, glu_act], 0).astype(jnp.float32)
        conv_out = jnp.zeros(glu_act.shape, jnp.float32)
        for offset in range(CONV_WIDTH):
            conv_out = conv_out + taps[layer, offset] * padded[offset : offset + rows]
        row_sum, row_square = lax.psum(
            (jnp.sum(conv_out, -1, keepdims=True), jnp.sum(conv_out * conv_out, -1, keepdims=True)),
            "tp",
        )
        center = row_sum / D
        spread = jnp.maximum(row_square / D - center * center, 0.0)
        activated = jax.nn.silu(
            (conv_out - center) * lax.rsqrt(spread + LN_EPSILON) * norm_gain[layer]
            + norm_shift[layer]
        ).astype(jnp.bfloat16)
        terms = jnp.dot(activated, out_mat, preferred_element_type=jnp.float32)
        summed = lax.psum_scatter(terms.astype(jnp.bfloat16), "tp", scatter_dimension=1, tiled=True)
        projected = summed.astype(jnp.float32)
        out_square = lax.psum(jnp.sum(projected * projected, -1, keepdims=True), "tp")
        scale = lax.rsqrt(out_square / D + EPSILON)
        stream = (stream.astype(jnp.float32) + projected * scale * post_gain[layer]).astype(
            jnp.bfloat16
        )
    return stream


TILE = 64
PACK = 16
HALO = 32
DIAGONAL_FIRST_X = ((True, True), (True, False))
DIAGONAL_X = (True, True)


def step(
    x_ref, pre_ref, wv_hbm, wg_hbm, taps_ref, ng_ref, ns_ref, wo_hbm, post_ref, out_ref,
    weight, other, whole, shared, normed, glu, conv, act, part_out, part_in, x_out, x_in, z_out, z_in,
    total, taps, gain, shift, stat, stat_in, post_all, local_sem,
    zs, zr, ys, yr, gs, gr, fs, fr, hs, hr, ss, sr, ps, pr, xs, xr, bs, br, qs, qr,
):
    sp, tp = lax.axis_index("sp"), lax.axis_index("tp")
    rows, cols = x_ref.shape
    layers = pre_ref.shape[0]
    nsp, ntp = 8, 4
    z, y = sp // 2, sp % 2
    zh, zl = z // 2, z % 2
    x, c = tp // 2, tp % 2
    plane = [z, zh * 2 + 1 - zl, (1 - zh) * 2 + zl, (1 - zh) * 2 + 1 - zl]
    partner = plane[1] * 2 + y
    beside, facing = (partner, tp), (z * 2 + 1 - y, tp)
    mate, across, diagonal = (sp, x * 2 + 1 - c), (sp, (1 - x) * 2 + c), (sp, (1 - x) * 2 + 1 - c)
    units = 3 * layers
    both, half = 2 * rows, cols // 2
    mine = pl.ds(pl.multiple_of(zl * half, half), half)
    rest = pl.ds(pl.multiple_of((1 - zl) * half, half), half)
    depth = wv_hbm.shape[1]

    def copy(src, dst, send, recv, to):
        return pltpu.make_async_remote_copy(
            src_ref=src, dst_ref=dst, send_sem=send, recv_sem=recv, device_id=to,
            device_id_type=pl.DeviceIdType.MESH,
        )

    def piece(u, slot):
        return weight.at[u, pl.ds(pl.multiple_of(slot * depth, depth), depth)]

    def along(u, k):
        p = piece(u, sp)
        return copy(
            p if k == 2 else other.at[u], p, zs.at[u, k - 1], zr.at[u, k - 1], (plane[k] * 2 + y, tp)
        )

    def sideways(u, k):
        p = piece(u, plane[k] * 2 + y)
        return copy(p, p, ys.at[u, k], yr.at[u, k], facing)

    def own(u):
        for k in (1, 2, 3):
            along(u, k).start()

    def relay(u, k):
        p = piece(u, plane[k] * 2 + y)
        copy(p, p, zs.at[u, k - 1], zr.at[u, k - 1], beside).wait_recv()
        sideways(u, k).start()

    def arrive(u):
        for k in range(4):
            p = piece(u, plane[k] * 2 + 1 - y)
            copy(p, p, ys.at[u, k], yr.at[u, k], facing).wait_recv()

    here, there = zl * 4, (1 - zl) * 4
    opposite = (1 - x) * 2 + c

    upper, lower = pl.ds(0, rows // 2), pl.ds(rows // 2, rows // 2)
    full = pl.ds(0, rows)
    routes = dict(
        across=(here + tp, full, across),
        beside_upper=(here + tp, upper, beside),
        beside_lower=(here + tp, lower, beside),
        mate=(here + tp, full, mate),
        diagonal_upper=(there + tp, upper, across),
        diagonal_lower=(there + tp, lower, across),
        across_mate=(here + opposite, full, mate),
        beside_mate=(there + tp, full, mate),
        both_mate_upper=(there + opposite, upper, mate),
        both_mate_lower=(there + opposite, lower, mate),
    )

    def gather(name):
        k = list(routes).index(name)
        t, part, to = routes[name]
        b = whole.at[0, t, part]
        return copy(b, b, gs.at[k], gr.at[k], to)

    def came(name, t):
        k = list(routes).index(name)
        b = whole.at[0, t, routes[name][1]]
        copy(b, b, gs.at[k], gr.at[k], mate).wait_recv()

    def gather_start():
        for name in ("across", "beside_upper", "beside_lower", "mate"):
            gather(name).start()

    def gather_upper():
        came("beside_upper", there + tp)
        gather("diagonal_upper").start()

    def gather_lower():
        came("beside_lower", there + tp)
        gather("diagonal_lower").start()
        gather("beside_mate").start()

    def gather_across():
        came("across", here + opposite)
        gather("across_mate").start()

    def gather_last():
        came("diagonal_upper", there + opposite)
        gather("both_mate_upper").start()
        came("diagonal_lower", there + opposite)
        gather("both_mate_lower").start()

    pair_tp, pair_opposite = x * 2 + 1 - c, (1 - x) * 2 + 1 - c
    tiles = rows // TILE

    def row_scale(square):
        return lax.rsqrt(square / (cols * ntp) + EPSILON)

    def norm():
        came("mate", here + pair_tp)
        came("across_mate", here + pair_opposite)
        came("beside_mate", there + pair_tp)
        came("both_mate_upper", there + pair_opposite)
        came("both_mate_lower", there + pair_opposite)

        @pl.loop(0, 2 * tiles)
        def _(i):
            g, r = i // tiles * 4, pl.ds(pl.multiple_of(i % tiles * TILE, TILE), TILE)
            to = pl.ds(pl.multiple_of(i * TILE, TILE), TILE)
            square = jnp.zeros((TILE, 1), jnp.float32)
            for t in range(ntp):
                v = whole[0, g + t, r, :].astype(jnp.float32)
                square = square + jnp.sum(v * v, -1, keepdims=True)
            scale = row_scale(square)
            for t in range(ntp):
                v = whole[0, g + t, r, :].astype(jnp.float32)
                at = slice(t * cols, (t + 1) * cols)
                normed[to, at] = (v * scale * pre_ref[0:1, at]).astype(jnp.bfloat16)

    hand = [
        dict(
            across=(here + tp, across, here + opposite),
            beside=(here + tp, beside, there + tp),
            mate=(here + tp, mate, here + pair_tp),
            diagonal=(
                (there + tp if DIAGONAL_X[h] else here + opposite),
                (across if DIAGONAL_X[h] else beside),
                there + opposite,
            ),
            across_mate=(here + opposite, mate, here + pair_opposite),
            beside_mate=(there + tp, mate, there + pair_tp),
            both_mate=(there + opposite, mate, there + pair_opposite),
        )
        for h in range(2)
    ]

    def share(l, name, h):
        k = list(hand[h]).index(name) * 2 + h
        t, to, _ = hand[h][name]
        b = shared.at[l, t, h]
        return copy(b, b, fs.at[l, k], fr.at[l, k], to)

    def shared_wait(l, name, h):
        k = list(hand[h]).index(name) * 2 + h
        b = shared.at[l, hand[h][name][2], h]
        copy(b, b, fs.at[l, k], fr.at[l, k], mate).wait_recv()

    def share_start(l, h):
        for name in ("across", "beside", "mate"):
            share(l, name, h).start()

    def share_turn(l, name, h):
        shared_wait(l, name, h)
        if (name == "beside") == DIAGONAL_X[h]:
            share(l, "diagonal", h).start()
        share(l, name + "_mate", h).start()

    def share_last(l, h):
        shared_wait(l, "diagonal", h)
        share(l, "both_mate", h).start()

    def post_copy(j):
        return copy(post_ref, post_all.at[tp], qs.at[j], qr.at[j], (mate, across, diagonal)[j])

    def post_wait(j):
        t = (pair_tp, opposite, pair_opposite)[j]
        copy(post_ref, post_all.at[t], qs.at[j], qr.at[j], mate).wait_recv()

    def norm_next(l):
        for h in range(per):
            for name in ("mate", "across_mate", "beside_mate", "both_mate"):
                shared_wait(l, name, h)

        @pl.loop(0, 2 * tiles)
        def _(i):
            g, r = i // tiles * 4, pl.ds(pl.multiple_of(i % tiles * TILE, TILE), TILE)
            to = pl.ds(pl.multiple_of(i * TILE, TILE), TILE)
            square = jnp.zeros((TILE, 1), jnp.float32)
            for t in range(ntp):
                for h in range(per):
                    v = shared[l, g + t, h, r, :].astype(jnp.float32)
                    square = square + jnp.sum(v * v, -1, keepdims=True)
            scale = row_scale(square)
            square = jnp.zeros((TILE, 1), jnp.float32)
            for t in range(ntp):
                for h in range(per):
                    at = slice(h * each, (h + 1) * each)
                    v = shared[l, g + t, h, r, :].astype(jnp.float32)
                    old = whole[l, g + t, r, at].astype(jnp.float32)
                    new = (old + v * scale * post_all[t, l : l + 1, at]).astype(jnp.bfloat16)
                    whole[l + 1, g + t, r, at] = new
                    v = new.astype(jnp.float32)
                    square = square + jnp.sum(v * v, -1, keepdims=True)
            scale = row_scale(square)
            for t in range(ntp):
                v = whole[l + 1, g + t, r, :].astype(jnp.float32)
                at = slice(t * cols, (t + 1) * cols)
                normed[to, at] = (v * scale * pre_ref[l + 1 : l + 2, at]).astype(jnp.bfloat16)

    tail, head = pl.ds(rows, HALO), pl.ds(0, HALO)

    def near_halo(l):
        return copy(glu.at[l, 0, tail], glu.at[l, y, head], hs.at[l, 0], hr.at[l, y], facing)

    def even_halo(l):
        return copy(glu.at[l, 1, tail], glu.at[l, 1, head], hs.at[l, 1], hr.at[l, 1], facing)

    def odd_halo(l):
        return copy(
            glu.at[l, 1, tail], glu.at[l, 0, head], hs.at[l, 1], hr.at[l, 0], ((z + 2) * 2, tp)
        )

    def halo_send(l, act_on):
        act_on(near_halo(l))
        pl.when(y == 0)(lambda: act_on(even_halo(l)))
        pl.when((y == 1) & (zh == 0))(lambda: act_on(odd_halo(l)))

    def halo_wait(l):
        def got(q):
            b = glu.at[l, q, head]
            copy(b, b, hs.at[l, q], hr.at[l, q], facing).wait_recv()

        pl.when((y == 1) | (zh == 1))(lambda: got(0))
        got(1)

        @pl.when((y == 0) & (zh == 0))
        def _():
            glu[l, 0, :HALO] = jnp.zeros((HALO, half), jnp.bfloat16)

    def project(l):
        n = normed[...]
        value = jnp.dot(n, weight[3 * l], preferred_element_type=jnp.float32)
        gate = jnp.dot(n, weight[3 * l + 1], preferred_element_type=jnp.float32)
        made = (value * jax.nn.sigmoid(gate)).astype(jnp.bfloat16)
        glu[l, 0, HALO:, :] = made[:rows]
        glu[l, 1, HALO:, :] = made[rows:]
        halo_send(l, lambda h: h.start())

    peers = [mate, across, diagonal, beside]
    peers += [(partner, mate[1]), (partner, across[1]), (partner, diagonal[1])]

    def exchange(e):
        return [
            copy(stat.at[e], stat_in.at[e, j], ss.at[e, j], sr.at[e, j], to)
            for j, to in enumerate(peers[: 3 if e % 2 else 7])
        ]

    def exchanged(e):
        sums = stat[e]
        for j, s in enumerate(exchange(e)):
            s.wait_recv()
            sums = sums + stat_in[e, j]
        return sums

    lane = lax.broadcasted_iota(jnp.int32, (PACK, 128), 1)
    groups = TILE // PACK

    def pick(sums, at):
        found = [
            jnp.sum(jnp.where(lane == at * groups + g, sums, 0.0), -1, keepdims=True)
            for g in range(groups)
        ]
        return jnp.concatenate(found, 0)

    def pack(sums, at, column):
        for g in range(groups):
            sums = jnp.where(lane == at * groups + g, column[g * PACK : (g + 1) * PACK], sums)
        return sums

    def convolve(l):
        first = HALO - (CONV_WIDTH - 1)

        def tile(q, i, sums):
            r = pl.multiple_of(i * TILE, TILE)
            one = jnp.zeros((TILE, 128), jnp.float32)
            two = jnp.zeros((TILE, 128), jnp.float32)
            for j in range(half // 128):
                at = slice(j * 128, (j + 1) * 128)
                window = glu[l, q, pl.ds(r, TILE + HALO), at].astype(jnp.float32)
                acc = jnp.zeros((TILE, 128), jnp.float32)
                for s in range(8):
                    w = window if s == 0 else pltpu.roll(window, TILE + HALO - s, 0)
                    for k in range(CONV_WIDTH):
                        if (first + k) % 8 == s:
                            o = first + k - s
                            acc = acc + taps[l, k : k + 1, at] * w[o : o + TILE]
                conv[q, pl.ds(r, TILE), at] = acc
                one = one + acc
                two = two + acc * acc
            n = q * tiles + i
            sums = pack(sums, 2 * n, jnp.sum(one, -1, keepdims=True))
            return pack(sums, 2 * n + 1, jnp.sum(two, -1, keepdims=True))

        inner = tiles - 1
        sums = lax.fori_loop(
            0, 2 * inner, lambda i, s: tile(i // inner, i % inner + 1, s),
            jnp.zeros((PACK, 128), jnp.float32),
        )
        halo_wait(l)
        stat[2 * l] = lax.fori_loop(0, 2, lambda q, s: tile(q, 0, s), sums)
        for s in exchange(2 * l):
            s.start()

    def activate(l, q):
        sums = stat[2 * l]
        for j in range(7):
            sums = sums + stat_in[2 * l, j]

        @pl.loop(0, tiles)
        def _(i):
            at, r = q * tiles + i, pl.ds(pl.multiple_of(i * TILE, TILE), TILE)
            center = pick(sums, 2 * at) / (cols * ntp)
            spread = jnp.maximum(pick(sums, 2 * at + 1) / (cols * ntp) - center * center, 0.0)
            v = (conv[q, r, :] - center) * lax.rsqrt(spread + LN_EPSILON)
            v = v * gain[l : l + 1, :] + shift[l : l + 1, :]
            act[q, r, :] = (v * jax.nn.sigmoid(v)).astype(jnp.bfloat16)

    def moments(l):
        for s in exchange(2 * l):
            s.wait_recv()

    each = wo_hbm.shape[2]
    per = cols // each
    quads = dict(D=(1 - zl, 1 - x), A=(zl, 1 - x), B=(1 - zl, x), O=(zl, x))
    names = list(quads)

    def term(l, quad, h, core):
        q, column = quads[quad]
        slot = (column * 2 + core) * per + h
        w = weight[3 * l + 2, pl.ds(pl.multiple_of(slot * depth, depth), depth), :]
        return jnp.dot(act[q], w, preferred_element_type=jnp.float32).astype(jnp.bfloat16)

    def pair(l, quad, h):
        i = names.index(quad) * per + h
        return copy(part_out.at[l, i], part_in.at[l, i], ps.at[l, i], pr.at[l, i], mate)

    def over(l, i):
        return copy(x_out.at[l, i], x_in.at[l, i], xs.at[l, i], xr.at[l, i], across)

    def along_pair(l, i):
        return copy(z_out.at[l, i], z_in.at[l, i], bs.at[l, i], br.at[l, i], beside)

    def give(l, quad, h):
        part_out[l, names.index(quad) * per + h] = term(l, quad, h, 1 - c)
        pair(l, quad, h).start()

    def joined(l, quad, h):
        kept = term(l, quad, h, c).astype(jnp.float32)
        pair(l, quad, h).wait_recv()
        return kept + part_in[l, names.index(quad) * per + h].astype(jnp.float32)

    def pass_x(l, i, v):
        x_out[l, i] = v.astype(jnp.bfloat16)
        over(l, i).start()

    def pass_z(l, i, v):
        z_out[l, i] = v.astype(jnp.bfloat16)
        along_pair(l, i).start()

    def move_on(l, quad, h):
        v = joined(l, quad, h)
        if quad == "O":
            total[:, h * each : (h + 1) * each] = v
        elif quad == "A":
            if not DIAGONAL_FIRST_X[l][h]:
                along_pair(l, h).wait_recv()
                v = v + z_in[l, h].astype(jnp.float32)
            pass_x(l, 2 + h, v)
        elif quad == "B":
            if DIAGONAL_FIRST_X[l][h]:
                over(l, h).wait_recv()
                v = v + x_in[l, h].astype(jnp.float32)
            pass_z(l, 2 + h, v)
        elif DIAGONAL_FIRST_X[l][h]:
            pass_x(l, h, v)
        else:
            pass_z(l, h, v)

    def steps(l, names):
        for name in names.split():
            (give if name[0] == "g" else move_on)(l, name[1], int(name[2]))

    def projected(l, h, r):
        at = slice(h * each, (h + 1) * each)
        p = total[r, at] + x_in[l, 2 + h, r, :].astype(jnp.float32)
        return (p + z_in[l, 2 + h, r, :].astype(jnp.float32)).astype(jnp.bfloat16)

    def settle(l, h):
        over(l, 2 + h).wait_recv()
        along_pair(l, 2 + h).wait_recv()

        @pl.loop(0, tiles)
        def _(i):
            r = pl.ds(pl.multiple_of(i * TILE, TILE), TILE)
            shared[l, here + tp, h, r, :] = projected(l, h, r)

        share_start(l, h)

    def finish(l):
        for h in range(per):
            over(l, 2 + h).wait_recv()
            along_pair(l, 2 + h).wait_recv()

        def tile(i, sums):
            r = pl.ds(pl.multiple_of(i * TILE, TILE), TILE)
            square = jnp.zeros((TILE, 1), jnp.float32)
            for h in range(per):
                p = projected(l, h, r).astype(jnp.float32)
                total[r, h * each : (h + 1) * each] = p
                square = square + jnp.sum(p * p, -1, keepdims=True)
            return pack(sums, i, square)

        e = 2 * l + 1
        stat[e] = lax.fori_loop(0, tiles, tile, jnp.zeros((PACK, 128), jnp.float32))
        for s in exchange(e):
            s.start()
        sums = exchanged(e)

        @pl.loop(0, tiles)
        def _(i):
            r = pl.ds(pl.multiple_of(i * TILE, TILE), TILE)
            old = whole[l, here + tp, r, :].astype(jnp.float32)
            new = old + total[r, :] * row_scale(pick(sums, i)) * post_ref[l : l + 1, :]
            out_ref[r, :] = new.astype(jnp.bfloat16)

    held = [pltpu.make_async_copy(x_ref, whole.at[0, here + tp], local_sem.at[2 * units])]
    for u in range(units):
        l, kind = divmod(u, 3)
        ref = (wv_hbm, wg_hbm, wo_hbm)[kind]
        for i, (part, to) in enumerate(((mine, piece(u, sp)), (rest, other.at[u]))):
            src = ref.at[l, part] if kind == 2 else ref.at[l, :, part]
            held.append(pltpu.make_async_copy(src, to, local_sem.at[2 * u + i]))
    for h in held:
        h.start()
    post_all[tp] = post_ref[...]
    for l in range(layers):
        taps[l] = taps_ref[:, l, mine]
        gain[l : l + 1] = ng_ref[l : l + 1, mine]
        shift[l : l + 1] = ns_ref[l : l + 1, mine]
    barrier = pltpu.get_barrier_semaphore()
    for i in range(1, nsp):
        pl.semaphore_signal(
            barrier, inc=1, device_id=(lax.rem(sp + i, nsp), tp),
            device_id_type=pl.DeviceIdType.MESH,
        )
    for i in range(1, ntp):
        for at in (sp, partner):
            pl.semaphore_signal(
                barrier, inc=1, device_id=(at, lax.rem(tp + i, ntp)),
                device_id_type=pl.DeviceIdType.MESH,
            )
    pl.semaphore_wait(barrier, nsp - 1 + 2 * (ntp - 1))
    for h in held:
        h.wait()

    far = range(1, 4)
    own(0)
    sideways(0, 0).start()
    gather_start()
    for j in range(3):
        post_copy(j).start()
    own(1)
    sideways(1, 0).start()
    for k in far:
        relay(0, k)
    gather_upper()
    relay(1, 2)
    gather_lower()
    relay(1, 3)
    gather_across()
    own(2)
    relay(1, 1)
    sideways(2, 0).start()
    gather_last()
    norm()
    arrive(0)
    arrive(1)
    project(0)
    relay(2, 1)
    relay(2, 2)
    convolve(0)
    own(3)
    own(4)
    relay(2, 3)
    moments(0)
    activate(0, 1 - zl)
    arrive(2)
    steps(0, "gD0 gD1 mD0 mD1")
    activate(0, zl)
    steps(0, "gA0 gA1 gB0 gB1 mA0 mA1 gO0 gO1 mB0 mB1 mO0 mO1")
    sideways(3, 0).start()
    for k in far:
        relay(3, k)
    settle(0, 0)
    settle(0, 1)
    own(5)
    sideways(4, 0).start()
    share_turn(0, "beside", 0)
    for k in far:
        relay(4, k)
    share_turn(0, "beside", 1)
    share_turn(0, "across", 0)
    share_turn(0, "across", 1)
    sideways(5, 0).start()
    share_last(0, 0)
    share_last(0, 1)
    for j in range(3):
        post_wait(j)
    norm_next(0)
    arrive(3)
    arrive(4)
    project(1)
    for k in far:
        relay(5, k)
    convolve(1)
    moments(1)
    activate(1, 1 - zl)
    arrive(5)
    steps(1, "gD0 gD1 mD0 mD1")
    activate(1, zl)
    steps(1, "gA0 gB1 gA1 gB0 mA0 mB1 gO0 gO1 mO0 mO1 mA1 mB0")
    finish(1)

    sent = [along(u, k) for u in range(units) for k in far]
    sent += [sideways(u, k) for u in range(units) for k in range(4)]
    sent += [gather(name) for name in routes] + [post_copy(j) for j in range(3)]
    for l in range(layers):
        sent += exchange(2 * l)
        if l + 1 < layers:
            sent += [share(l, name, h) for h in range(per) for name in hand[h]]
        else:
            sent += exchange(2 * l + 1)
        for h in range(per):
            sent += [over(l, 2 + h), along_pair(l, 2 + h)]
            sent.append(over(l, h) if DIAGONAL_FIRST_X[l][h] else along_pair(l, h))
            sent += [pair(l, quad, h) for quad in names]
        halo_send(l, lambda h: h.wait_send())
    for s in sent:
        s.wait_send()


def kernel_local(*args):
    tokens, pre_gain, w_value, w_gate, all_taps, norm_gain, norm_shift, w_out, post_gain = args
    rows, cols = tokens.shape
    layers, depth = w_value.shape[:2]
    each = w_out.shape[2]
    half, units = cols // 2, 3 * layers
    if rows % TILE or 2 * 2 * rows > PACK * 128 or not depth == half == each:
        return local(*args)
    vmem, hbm = pl.BlockSpec(memory_space=pltpu.VMEM), pl.BlockSpec(memory_space=pl.ANY)
    bf16, f32, dma = jnp.bfloat16, jnp.float32, pltpu.SemaphoreType.DMA
    return pl.pallas_call(
        step,
        out_shape=jax.ShapeDtypeStruct((rows, cols), bf16),
        in_specs=[hbm, vmem, hbm, hbm, vmem, vmem, vmem, hbm, vmem],
        out_specs=vmem,
        scratch_shapes=[
            pltpu.VMEM((units, 8 * depth, half), bf16),
            pltpu.VMEM((units, depth, half), bf16),
            pltpu.VMEM((layers, 8, rows, cols), bf16),
            pltpu.VMEM((layers - 1, 8, 2, rows, each), bf16),
            pltpu.VMEM((2 * rows, 4 * cols), bf16),
            pltpu.VMEM((layers, 2, HALO + rows, half), bf16),
            pltpu.VMEM((2, rows, half), f32),
            pltpu.VMEM((2, rows, half), bf16),
            pltpu.VMEM((layers, 8, rows, each), bf16),
            pltpu.VMEM((layers, 8, rows, each), bf16),
            pltpu.VMEM((layers, 4, rows, each), bf16),
            pltpu.VMEM((layers, 4, rows, each), bf16),
            pltpu.VMEM((layers, 4, rows, each), bf16),
            pltpu.VMEM((layers, 4, rows, each), bf16),
            pltpu.VMEM((rows, cols), f32),
            pltpu.VMEM((layers, CONV_WIDTH, half), f32),
            pltpu.VMEM((layers, half), f32),
            pltpu.VMEM((layers, half), f32),
            pltpu.VMEM((2 * layers, PACK, 128), f32),
            pltpu.VMEM((2 * layers, 7, PACK, 128), f32),
            pltpu.VMEM((4, layers, cols), f32),
            dma((2 * units + 1,)),
            dma((units, 3)), dma((units, 3)),
            dma((units, 4)), dma((units, 4)),
            dma((10,)), dma((10,)),
            dma((layers - 1, 14)), dma((layers - 1, 14)),
            dma((layers, 2)), dma((layers, 2)),
            dma((2 * layers, 7)), dma((2 * layers, 7)),
            dma((layers, 8)), dma((layers, 8)),
            dma((layers, 4)), dma((layers, 4)),
            dma((layers, 4)), dma((layers, 4)),
            dma((3,)), dma((3,)),
        ],
        compiler_params=pltpu.CompilerParams(
            collective_id=0, has_side_effects=True, vmem_limit_bytes=56 * 1024 * 1024
        ),
    )(
        tokens, pre_gain, w_value, w_gate, jnp.swapaxes(all_taps, 0, 1), norm_gain, norm_shift, w_out,
        post_gain,
    )


def solution(mesh):
    nsp, ntp = mesh.shape["sp"], mesh.shape["tp"]
    body = kernel_local if nsp == 8 and ntp == 4 else local
    placed = (
        P("sp", "tp"),
        P(),
        P(None, "sp", "tp"),
        P(None, "sp", "tp"),
        P(None, None, "tp"),
        P(None, "tp"),
        P(None, "tp"),
        P(None, "tp", "sp"),
        P(None, "tp"),
    )
    return jax.shard_map(
        body, mesh=mesh, in_specs=placed, out_specs=P("sp", "tp"), check_vma=False
    )
```

```python
import jax
import jax.numpy as jnp
from jax import lax
from jax.experimental import pallas as pl
from jax.experimental.pallas import tpu as pltpu
from jax.sharding import PartitionSpec as P

D = 2048
CONV_WIDTH = 31
LAYERS = 2


EPSILON = 1e-06
LN_EPSILON = 1e-05


def passed_along(block, axis, distance):
    devices = range(lax.axis_size(axis))
    route = [(i - distance, i) for i in devices if i - distance in devices]
    return lax.ppermute(block, axis, route)


def local(tokens, pre_gain, w_value, w_gate, taps, norm_gain, norm_shift, w_out, post_gain):
    stream = tokens
    full_value, full_gate = (
        lax.all_gather(w_value, "sp", axis=1, tiled=True),
        lax.all_gather(w_gate, "sp", axis=1, tiled=True),
    )
    full_out = lax.all_gather(w_out, "sp", axis=2, tiled=True)
    for layer in range(LAYERS):
        whole = lax.all_gather(stream, "tp", axis=1, tiled=True)
        whole_f = whole.astype(jnp.float32)
        normed = (
            whole_f
            * lax.rsqrt(jnp.mean(whole_f * whole_f, -1, keepdims=True) + EPSILON)
            * pre_gain[layer]
        ).astype(jnp.bfloat16)
        value_mat = full_value[layer]
        gate_mat = full_gate[layer]
        out_mat = full_out[layer]
        value_proj = jnp.dot(normed, value_mat, preferred_element_type=jnp.float32)
        gate_proj = jnp.dot(normed, gate_mat, preferred_element_type=jnp.float32)
        glu_act = (value_proj * jax.nn.sigmoid(gate_proj)).astype(jnp.bfloat16)
        rows = glu_act.shape[0]
        fringe = passed_along(glu_act[rows - (CONV_WIDTH - 1) :], "sp", 1)
        padded = jnp.concatenate([fringe, glu_act], 0).astype(jnp.float32)
        conv_out = jnp.zeros(glu_act.shape, jnp.float32)
        for offset in range(CONV_WIDTH):
            conv_out = conv_out + taps[layer, offset] * padded[offset : offset + rows]
        row_sum, row_square = lax.psum(
            (jnp.sum(conv_out, -1, keepdims=True), jnp.sum(conv_out * conv_out, -1, keepdims=True)),
            "tp",
        )
        center = row_sum / D
        spread = jnp.maximum(row_square / D - center * center, 0.0)
        activated = jax.nn.silu(
            (conv_out - center) * lax.rsqrt(spread + LN_EPSILON) * norm_gain[layer]
            + norm_shift[layer]
        ).astype(jnp.bfloat16)
        terms = jnp.dot(activated, out_mat, preferred_element_type=jnp.float32)
        summed = lax.psum_scatter(terms.astype(jnp.bfloat16), "tp", scatter_dimension=1, tiled=True)
        projected = summed.astype(jnp.float32)
        out_square = lax.psum(jnp.sum(projected * projected, -1, keepdims=True), "tp")
        scale = lax.rsqrt(out_square / D + EPSILON)
        stream = (stream.astype(jnp.float32) + projected * scale * post_gain[layer]).astype(
            jnp.bfloat16
        )
    return stream


TILE = 64
PACK = 16
HALO = 32
OVER_X = ((True, True), (True, False))
FAR = (1, 2, 3)


def step(
    x_ref, pre_ref, wv_hbm, wg_hbm, taps_ref, ng_ref, ns_ref, wo_hbm, post_ref, out_ref,
    weight, other, whole, shared, stream, normed, fresh, kept, added, row_sums, row_moments, glu, conv, act,
    part_out, part_in, x_out, x_in, z_out, z_in, total, held,
    taps, gain, shift, pre_all, post_all, stat, stat_in, local_sem,
    zs, zr, ys, yr, gs, gr, fs, fr, hs, hr, ss, sr, ps, pr, xs, xr, bs, br, qs, qr,
):
    sp, tp = lax.axis_index("sp"), lax.axis_index("tp")
    rows, cols = x_ref.shape
    layers, units, nsp, ntp = 2, 6, 8, 4
    z, y = sp // 2, sp % 2
    zh, zl = z // 2, z % 2
    x, c = tp // 2, tp % 2
    plane = [z, zh * 2 + 1 - zl, (1 - zh) * 2 + zl, (1 - zh) * 2 + 1 - zl]
    partner = plane[1] * 2 + y
    beside, facing = (partner, tp), (z * 2 + 1 - y, tp)
    mate, across, diagonal = (sp, x * 2 + 1 - c), (sp, (1 - x) * 2 + c), (sp, (1 - x) * 2 + 1 - c)
    both, half, tiles = 2 * rows, cols // 2, rows // TILE
    mine = pl.ds(pl.multiple_of(zl * half, half), half)
    rest = pl.ds(pl.multiple_of((1 - zl) * half, half), half)
    depth, each = wv_hbm.shape[1], wo_hbm.shape[2]
    per = cols // each

    def copy(src, dst, send, recv, to):
        return pltpu.make_async_remote_copy(
            src_ref=src, dst_ref=dst, send_sem=send, recv_sem=recv, device_id=to,
            device_id_type=pl.DeviceIdType.MESH,
        )

    def took(b, sem):
        copy(b, b, sem, sem, mate).wait_recv()

    def left(b, sem):
        copy(b, b, sem, sem, mate).wait_send()

    def block(i, size=TILE):
        if isinstance(i, int):
            return pl.ds(i * size, size)
        return pl.ds(pl.multiple_of(i * size, size), size)

    def piece(u, slot):
        return weight.at[u, block(slot, depth)]

    def landing(u, k):
        return zr.at[u * 3 + k - 1]

    def along(u, k):
        p = piece(u, sp)
        src = p if k == 2 else other.at[u]
        return copy(src, p, zs.at[k - 1], landing(u, k), (plane[k] * 2 + y, tp))

    def own(u):
        for k in FAR:
            along(u, k).start()

    def sideways(u, k):
        p = piece(u, plane[k] * 2 + y)
        copy(p, p, ys.at[0], yr.at[u], facing).start()

    def relay(u, *ks):
        for k in ks:
            took(piece(u, plane[k] * 2 + y), landing(u, k))
            sideways(u, k)

    def relay_near(u):
        pl.when(zl == zh)(lambda: relay(u, 2))
        pl.when(zl != zh)(lambda: relay(u, 3))

    def relay_far(u):
        pl.when(zl == zh)(lambda: relay(u, 3))
        pl.when(zl != zh)(lambda: relay(u, 2))

    def arrive(u):
        took(weight.at[u, : 4 * depth], yr.at[u])

    here, there = zl * 4, (1 - zl) * 4
    opposite = (1 - x) * 2 + c
    upper, lower = pl.ds(0, rows // 2), pl.ds(rows // 2, rows // 2)
    full = pl.ds(0, rows)
    routes = dict(
        across=(here + tp, full, across, 0),
        beside_upper=(here + tp, upper, beside, 1),
        beside_lower=(here + tp, lower, beside, 2),
        mate=(here + tp, full, mate, 5),
        diagonal_upper=(there + tp, upper, across, 3),
        diagonal_lower=(there + tp, lower, across, 4),
        across_mate=(here + opposite, full, mate, 5),
        beside_mate=(there + tp, full, mate, 5),
        both_mate_upper=(there + opposite, upper, mate, 5),
        both_mate_lower=(there + opposite, lower, mate, 5),
    )

    def gather(name):
        t, part, to, k = routes[name]
        b = whole.at[t, part]
        copy(b, b, gs.at[0], gr.at[k], to).start()

    def came(name, t):
        took(whole.at[t, routes[name][1]], gr.at[routes[name][3]])

    def gather_start():
        for name in ("across", "beside_upper", "beside_lower", "mate"):
            gather(name)

    def gather_upper():
        came("beside_upper", there + tp)
        gather("diagonal_upper")

    def gather_lower():
        came("beside_lower", there + tp)
        gather("diagonal_lower")
        gather("beside_mate")

    def gather_across():
        came("across", here + opposite)
        gather("across_mate")

    def gather_last():
        came("diagonal_upper", there + opposite)
        gather("both_mate_upper")
        came("diagonal_lower", there + opposite)
        gather("both_mate_lower")

    def row_scale(square):
        return lax.rsqrt(square / (cols * ntp) + EPSILON)

    def norm():
        took(whole.at[0:4], gr.at[5])

        @pl.loop(0, 2 * tiles)
        def _(i):
            g, r = i // tiles * 4, block(i % tiles)
            square = jnp.zeros((TILE, 1), jnp.float32)
            for t in range(ntp):
                v = whole[g + t, r, :].astype(jnp.float32)
                square = square + jnp.sum(v * v, -1, keepdims=True)
            scale = row_scale(square)
            for t in range(ntp):
                v = whole[g + t, r, :].astype(jnp.float32)
                at = slice(t * cols, (t + 1) * cols)
                normed[block(i), at] = (v * scale * pre_ref[0:1, at]).astype(jnp.bfloat16)

    def project_kept(l, kind):
        w = weight[3 * l + kind]
        for part in (slice(0, rows), slice(rows, both)):
            kept[kind, part] = jnp.dot(normed[part], w, preferred_element_type=jnp.float32)

    pair_tp, pair_opposite = x * 2 + 1 - c, (1 - x) * 2 + 1 - c
    hand = dict(
        across=(here + tp, across, here + opposite, 0),
        beside=(here + tp, beside, there + tp, 2),
        diagonal=(there + tp, across, there + opposite, 4),
        across_mate=(here + opposite, mate, here + pair_opposite, 6),
        beside_mate=(there + tp, mate, there + pair_tp, 8),
        both_mate=(there + opposite, mate, there + pair_opposite, 10),
        mate=(here + tp, mate, here + pair_tp, 12),
    )

    def share(name, h):
        t, to, _, k = hand[name]
        b = shared.at[t, h]
        copy(b, b, fs.at[0], fr.at[k if name == "mate" else k + h], to).start()

    def shared_wait(name, h):
        if name == "mate":
            took(shared.at[here + pair_tp], fr.at[12])
        else:
            took(shared.at[hand[name][2], h], fr.at[hand[name][3] + h])

    def share_turn(name, h):
        shared_wait(name, h)
        if name == "beside":
            share("diagonal", h)
        share("both_mate" if name == "diagonal" else name + "_mate", h)

    def keep_old():
        @pl.loop(0, 2 * tiles)
        def _(i):
            g, r = i // tiles * 4, block(i % tiles)
            square = jnp.zeros((TILE, 128), jnp.float32)
            for t in range(ntp):
                v = whole[g + t, r, :].astype(jnp.float32)
                at = slice(t * cols, (t + 1) * cols)
                normed[block(i), at] = (v * pre_ref[1:2, at]).astype(jnp.bfloat16)
                for j in range(cols // 128):
                    w = v[:, j * 128 : (j + 1) * 128]
                    square = square + w * w
            row_sums[3, block(i), :] = square

    groups_of = dict(
        mate=(zl, x), across_mate=(zl, 1 - x), beside_mate=(1 - zl, x), both_mate=(1 - zl, 1 - x)
    )
    begun = set()

    def fold(v):
        out = v[:, :128]
        for j in range(1, each // 128):
            out = out + v[:, j * 128 : (j + 1) * 128]
        return out

    def prepare(name, h):
        q, column = groups_of[name]
        side = name in ("mate", "across_mate")
        start = ("sums", side) not in begun
        begun.add(("sums", side))
        at = slice(h * each, (h + 1) * each)

        @pl.loop(0, tiles)
        def _(i):
            r, to = block(i), block(q * tiles + i)
            sums = [jnp.zeros((TILE, 128), jnp.float32) if start else row_sums[n, to, :] for n in range(3)]
            for core in range(2):
                t = column * 2 + core
                v = shared[q * 4 + t, h, r, :].astype(jnp.float32)
                old = whole[q * 4 + t, r, at].astype(jnp.float32)
                w = v * post_all[t, 0:1, at]
                fresh[q * 4 + t, h, r, :] = (w * pre_all[t, 1:2, at]).astype(jnp.bfloat16)
                sums = [s + fold(p) for s, p in zip(sums, (v * v, old * w, w * w))]
            for n in range(3):
                row_sums[n, to, :] = sums[n]

    def multiply(name, h, kinds=(0, 1)):
        q, column = groups_of[name]
        side, to = name in ("mate", "across_mate"), block(q, rows)
        sums = []
        for kind in kinds:
            v = None
            for core in range(2):
                t = column * 2 + core
                w = weight[3 + kind, block(t * per + h, depth), :]
                p = jnp.dot(fresh[q * 4 + t, h], w, preferred_element_type=jnp.float32)
                v = p if v is None else v + p
            sums.append(v)
        for kind, v in zip(kinds, sums):
            start = (kind, side) not in begun
            begun.add((kind, side))
            added[kind, to, :] = v if start else added[kind, to, :] + v

    def scales(to):
        new, cross, square, old = [
            jnp.sum(row_sums[n, to, :], -1, keepdims=True) for n in range(4)
        ]
        s = row_scale(new)
        return s, row_scale(jnp.maximum(old + 2.0 * s * cross + s * s * square, 0.0))

    def gate_tile(l, i):
        to = block(i)
        value, gate = kept[0, to, :], kept[1, to, :]
        if l:
            s, n = scales(to)
            value = n * (value + s * added[0, to, :])
            gate = n * (gate + s * added[1, to, :])
        made = (value * jax.nn.sigmoid(gate)).astype(jnp.bfloat16)
        glu[l, i // tiles, pl.ds(HALO + i % tiles * TILE, TILE), :] = made

    def project(l):
        inner = tiles - 1
        for q in range(2):
            gate_tile(l, q * tiles + inner)
        halo_send(l, lambda h: h.start())
        for i in range(2 * inner):
            gate_tile(l, i + i // inner)

    def new_stream():
        @pl.loop(0, tiles)
        def _(i):
            r = block(i)
            s, _ = scales(block(zl * tiles + i))
            for h in range(per):
                at = slice(h * each, (h + 1) * each)
                v = shared[here + tp, h, r, :].astype(jnp.float32)
                old = whole[here + tp, r, at].astype(jnp.float32)
                stream[r, at] = (old + v * s * post_ref[0:1, at]).astype(jnp.bfloat16)

    tail, head = pl.ds(rows, HALO), pl.ds(0, HALO)

    def near_halo(l):
        return copy(glu.at[l, 0, tail], glu.at[l, y, head], hs.at[l, 0], hr.at[l, y], facing)

    def even_halo(l):
        return copy(glu.at[l, 1, tail], glu.at[l, 1, head], hs.at[l, 1], hr.at[l, 1], facing)

    def odd_halo(l):
        return copy(
            glu.at[l, 1, tail], glu.at[l, 0, head], hs.at[l, 1], hr.at[l, 0], ((z + 2) * 2, tp)
        )

    def halo_send(l, act_on):
        act_on(near_halo(l))
        pl.when(y == 0)(lambda: act_on(even_halo(l)))
        pl.when((y == 1) & (zh == 0))(lambda: act_on(odd_halo(l)))

    def halo_wait(l):
        pl.when((y == 1) | (zh == 1))(lambda: took(glu.at[l, 0, head], hr.at[l, 0]))
        took(glu.at[l, 1, head], hr.at[l, 1])

        @pl.when((y == 0) & (zh == 0))
        def _():
            glu[l, 0, :HALO] = jnp.zeros((HALO, half), jnp.bfloat16)

    peers = [mate, across, diagonal, beside]
    peers += [(partner, mate[1]), (partner, across[1]), (partner, diagonal[1])]

    def exchange(e):
        for j, to in enumerate(peers[: 3 if e == layers else 7]):
            copy(stat.at[e], stat_in.at[e, j], ss.at[e], sr.at[e], to).start()

    def inbox(e):
        return stat_in.at[e, 0 : 3 if e == layers else 7]

    def received(e):
        sums = stat[e]
        for j in range(3 if e == layers else 7):
            sums = sums + stat_in[e, j]
        return sums

    lane = lax.broadcasted_iota(jnp.int32, (PACK, 128), 1)
    groups = TILE // PACK

    def pick(sums, at):
        found = [
            jnp.sum(jnp.where(lane == at * groups + g, sums, 0.0), -1, keepdims=True)
            for g in range(groups)
        ]
        return jnp.concatenate(found, 0)

    def pack(sums, at, column):
        for g in range(groups):
            sums = jnp.where(lane == at * groups + g, column[g * PACK : (g + 1) * PACK], sums)
        return sums

    def convolve(l):
        first = HALO - (CONV_WIDTH - 1)

        def tile(q, i):
            r = pl.multiple_of(i * TILE, TILE)
            one = jnp.zeros((TILE, 128), jnp.float32)
            two = jnp.zeros((TILE, 128), jnp.float32)
            for j in range(half // 128):
                at = slice(j * 128, (j + 1) * 128)
                window = glu[l, q, pl.ds(r, TILE + HALO), at].astype(jnp.float32)
                acc = jnp.zeros((TILE, 128), jnp.float32)
                for s in range(8):
                    w = window if s == 0 else pltpu.roll(window, TILE + HALO - s, 0)
                    for k in range(CONV_WIDTH):
                        if (first + k) % 8 == s:
                            o = first + k - s
                            acc = acc + taps[l, k : k + 1, at] * w[o : o + TILE]
                conv[q, pl.ds(r, TILE), at] = acc
                one = one + acc
                two = two + acc * acc
            row_moments[0, block(q * tiles + i), :] = one
            row_moments[1, block(q * tiles + i), :] = two

        inner = tiles - 1
        pl.loop(0, 2 * inner)(lambda i: tile(i // inner, i % inner + 1))
        halo_wait(l)
        pl.loop(0, 2)(lambda q: tile(q, 0))
        sums = jnp.zeros((PACK, 128), jnp.float32)
        for i in range(2 * tiles):
            for n in range(2):
                sums = pack(sums, 2 * i + n, jnp.sum(row_moments[n, block(i), :], -1, keepdims=True))
        stat[l] = sums
        exchange(l)

    def moments(l):
        took(inbox(l), sr.at[l])

    def activate(l, q):
        sums = received(l)

        for i in range(tiles):
            at, r = q * tiles + i, block(i)
            center = pick(sums, 2 * at) / (cols * ntp)
            spread = jnp.maximum(pick(sums, 2 * at + 1) / (cols * ntp) - center * center, 0.0)
            v = (conv[q, r, :] - center) * lax.rsqrt(spread + LN_EPSILON)
            v = v * gain[l : l + 1, :] + shift[l : l + 1, :]
            act[q, r, :] = (v * jax.nn.sigmoid(v)).astype(jnp.bfloat16)

    quads = dict(D=(1 - zl, 1 - x), A=(zl, 1 - x), B=(1 - zl, x), O=(zl, x))
    names = list(quads)

    def term(l, quad, h, core):
        q, column = quads[quad]
        w = weight[3 * l + 2, block((column * 2 + core) * per + h, depth), :]
        return jnp.dot(act[q], w, preferred_element_type=jnp.float32).astype(jnp.bfloat16)

    def give(l, quad):
        i = names.index(quad)
        made = [term(l, quad, h, 1 - c) for h in range(per)]
        for h in range(per):
            part_out[l, i, h] = made[h]
        copy(part_out.at[l, i], part_in.at[l, i], ps.at[l], pr.at[l, i], mate).start()

    def joined(l, quad):
        i = names.index(quad)
        made = [term(l, quad, h, c).astype(jnp.float32) for h in range(per)]
        took(part_in.at[l, i], pr.at[l, i])
        return [made[h] + part_in[l, i, h].astype(jnp.float32) for h in range(per)]

    def pass_x(l, i, v):
        x_out[l, i] = v.astype(jnp.bfloat16)
        copy(x_out.at[l, i], x_in.at[l, i], xs.at[l], xr.at[l, i], across).start()

    def pass_z(l, i, v):
        z_out[l, i] = v.astype(jnp.bfloat16)
        copy(z_out.at[l, i], z_in.at[l, i], bs.at[l], br.at[l, i], beside).start()

    def move_on(l, quad):
        for h, v in enumerate(joined(l, quad)):
            if quad == "O":
                total[:, h * each : (h + 1) * each] = v
            elif (quad == "A" and OVER_X[l][h]) or (quad == "D" and OVER_X[l][h]):
                pass_x(l, h if quad == "D" else 2 + h, v)
            elif quad == "D" or (quad == "B" and not OVER_X[l][h]):
                pass_z(l, h if quad == "D" else 2 + h, v)
            else:
                held[h] = v

    def pass_held(l, h):
        if OVER_X[l][h]:
            took(x_in.at[l, h], xr.at[l, h])
            pass_z(l, 2 + h, held[h] + x_in[l, h].astype(jnp.float32))
        else:
            took(z_in.at[l, h], br.at[l, h])
            pass_x(l, 2 + h, held[h] + z_in[l, h].astype(jnp.float32))

    def steps(l, *todo):
        for name in todo:
            (give if name[0] == "g" else move_on)(l, name[1])

    def projected(l, h, r):
        at = slice(h * each, (h + 1) * each)
        p = total[r, at] + x_in[l, 2 + h, r, :].astype(jnp.float32)
        return (p + z_in[l, 2 + h, r, :].astype(jnp.float32)).astype(jnp.bfloat16)

    def landed(l, h):
        took(x_in.at[l, 2 + h], xr.at[l, 2 + h])
        took(z_in.at[l, 2 + h], br.at[l, 2 + h])

    def settle(h):
        landed(0, h)

        @pl.loop(0, tiles)
        def _(i):
            shared[here + tp, h, block(i), :] = projected(0, h, block(i))

        for name in ("across", "beside", "mate"):
            share(name, h)

    def finish():
        l = layers - 1
        for h in range(per):
            landed(l, h)

        def tile(i, sums):
            r = block(i)
            square = jnp.zeros((TILE, 1), jnp.float32)
            for h in range(per):
                p = projected(l, h, r).astype(jnp.float32)
                total[r, h * each : (h + 1) * each] = p
                square = square + jnp.sum(p * p, -1, keepdims=True)
            return pack(sums, i, square)

        sums = jnp.zeros((PACK, 128), jnp.float32)
        for i in range(tiles):
            sums = tile(i, sums)
        stat[layers] = sums
        exchange(layers)
        took(inbox(layers), sr.at[layers])
        sums = received(layers)
        for i in range(tiles):
            r = block(i)
            new = total[r, :] * row_scale(pick(sums, i)) * post_ref[l : l + 1, :]
            out_ref[r, :] = (stream[r, :].astype(jnp.float32) + new).astype(jnp.bfloat16)

    pltpu.make_async_copy(x_ref, whole.at[here + tp], local_sem.at[2]).start()
    for u in range(units):
        l, kind = divmod(u, 3)
        ref = (wv_hbm, wg_hbm, wo_hbm)[kind]
        for i, (part, to) in enumerate(((mine, piece(u, sp)), (rest, other.at[u]))):
            src = ref.at[l, part] if kind == 2 else ref.at[l, :, part]
            pltpu.make_async_copy(src, to, local_sem.at[i]).start()
    post_all[tp] = post_ref[...]
    for t in range(ntp):
        pre_all[t] = pre_ref[:, t * cols : (t + 1) * cols]
    for l in range(layers):
        taps[l] = taps_ref[:, l, mine]
        gain[l : l + 1] = ng_ref[l : l + 1, mine]
        shift[l : l + 1] = ns_ref[l : l + 1, mine]
    barrier = pltpu.get_barrier_semaphore()
    for i in range(1, nsp):
        pl.semaphore_signal(
            barrier, inc=1, device_id=(lax.rem(sp + i, nsp), tp),
            device_id_type=pl.DeviceIdType.MESH,
        )
    for i in range(1, ntp):
        for at in (sp, partner):
            pl.semaphore_signal(
                barrier, inc=1, device_id=(at, lax.rem(tp + i, ntp)),
                device_id_type=pl.DeviceIdType.MESH,
            )
    pl.semaphore_wait(barrier, nsp - 1 + 2 * (ntp - 1))
    for i in range(2):
        pltpu.make_async_copy(other, other, local_sem.at[i]).wait()
    pltpu.make_async_copy(x_ref, whole.at[here + tp], local_sem.at[2]).wait()

    def post_start():
        for to in (mate, across, diagonal):
            copy(post_ref, post_all.at[tp], qs.at[0], qr.at[0], to).start()

    def post_wait():
        took(post_all.at[0:3], qr.at[0])

    own(0)
    sideways(0, 0)
    gather_start()
    post_start()
    own(1)
    sideways(1, 0)
    sideways(2, 0)
    relay_near(0)
    relay(0, 1)
    relay_far(0)
    gather_upper()
    relay_near(1)
    gather_lower()
    relay(1, 1)
    relay_far(1)
    gather_across()
    own(2)
    sideways(3, 0)
    gather_last()
    norm()
    arrive(0)
    project_kept(0, 0)
    arrive(1)
    project_kept(0, 1)
    project(0)
    convolve(0)
    own(3)
    own(4)
    relay_near(2)
    relay(2, 1)
    relay_far(2)
    sideways(4, 0)
    moments(0)
    activate(0, 1 - zl)
    arrive(2)
    steps(0, "gD")
    activate(0, zl)
    steps(0, "gA", "mD", "gB", "mA", "gO", "mB", "mO")
    pass_held(0, 0)
    pass_held(0, 1)
    relay(3, 1, 2, 3)
    post_wait()
    keep_old()
    settle(0)
    relay(4, 1)
    settle(1)
    own(5)
    relay(4, 2, 3)
    sideways(5, 0)
    arrive(3)
    project_kept(1, 0)
    shared_wait("mate", 0)
    prepare("mate", 0)
    prepare("mate", 1)
    share_turn("beside", 0)
    share_turn("across", 0)
    shared_wait("across_mate", 0)
    prepare("across_mate", 0)
    shared_wait("beside_mate", 0)
    prepare("beside_mate", 0)
    share_turn("beside", 1)
    share_turn("across", 1)
    arrive(4)
    project_kept(1, 1)
    share_turn("diagonal", 0)
    multiply("mate", 0)
    multiply("mate", 1)
    multiply("across_mate", 0)
    multiply("beside_mate", 0)
    shared_wait("across_mate", 1)
    prepare("across_mate", 1)
    multiply("across_mate", 1)
    shared_wait("beside_mate", 1)
    prepare("beside_mate", 1)
    multiply("beside_mate", 1)
    shared_wait("both_mate", 0)
    prepare("both_mate", 0)
    multiply("both_mate", 0)
    share_turn("diagonal", 1)
    relay(5, 1)
    shared_wait("both_mate", 1)
    prepare("both_mate", 1)
    multiply("both_mate", 1)
    project(1)
    relay(5, 2, 3)
    convolve(1)
    new_stream()
    moments(1)
    activate(1, 1 - zl)
    arrive(5)
    steps(1, "gD")
    activate(1, zl)
    steps(1, "gA", "mD", "gB", "mA", "gO", "mB", "mO")
    pass_held(1, 1)
    pass_held(1, 0)
    finish()
    for k in FAR:
        left(other, zs.at[k - 1])
    left(weight.at[0:3], ys.at[0])
    left(whole.at[0:7], gs.at[0])
    left(shared.at[0:7], fs.at[0])
    left(post_all.at[0:3], qs.at[0])
    for l in range(layers):
        left(inbox(l), ss.at[l])
        left(part_out.at[l], ps.at[l])
        left(x_out.at[l, 0 : 2 + sum(OVER_X[l])], xs.at[l])
        left(z_out.at[l, 0 : 4 - sum(OVER_X[l])], bs.at[l])
        halo_send(l, lambda h: h.wait_send())
    left(inbox(layers), ss.at[layers])


def kernel_local(*args):
    tokens, pre_gain, w_value, w_gate, all_taps, norm_gain, norm_shift, w_out, post_gain = args
    rows, cols = tokens.shape
    layers, depth = w_value.shape[:2]
    each = w_out.shape[2]
    half, units = cols // 2, 3 * layers
    square = depth == half == each and depth % 128 == 0
    if rows % TILE or 4 * rows > PACK * 128 or layers != 2 or not square:
        return local(*args)
    vmem, hbm = pl.BlockSpec(memory_space=pltpu.VMEM), pl.BlockSpec(memory_space=pl.ANY)
    bf16, f32, dma = jnp.bfloat16, jnp.float32, pltpu.SemaphoreType.DMA
    return pl.pallas_call(
        step,
        out_shape=pltpu.VMEM((rows, cols), bf16),
        in_specs=[hbm, vmem, hbm, hbm, vmem, vmem, vmem, hbm, vmem],
        out_specs=vmem,
        scratch_shapes=[
            pltpu.VMEM((units, 8 * depth, half), bf16),
            pltpu.VMEM((units, depth, half), bf16),
            pltpu.VMEM((8, rows, cols), bf16),
            pltpu.VMEM((8, 2, rows, each), bf16),
            pltpu.VMEM((rows, cols), bf16),
            pltpu.VMEM((2 * rows, 4 * cols), bf16),
            pltpu.VMEM((8, 2, rows, each), bf16),
            pltpu.VMEM((2, 2 * rows, half), f32),
            pltpu.VMEM((2, 2 * rows, half), f32),
            pltpu.VMEM((4, 2 * rows, 128), f32),
            pltpu.VMEM((2, 2 * rows, 128), f32),
            pltpu.VMEM((layers, 2, HALO + rows, half), bf16),
            pltpu.VMEM((2, rows, half), f32),
            pltpu.VMEM((2, rows, half), bf16),
            pltpu.VMEM((layers, 4, 2, rows, each), bf16),
            pltpu.VMEM((layers, 4, 2, rows, each), bf16),
            pltpu.VMEM((layers, 4, rows, each), bf16),
            pltpu.VMEM((layers, 4, rows, each), bf16),
            pltpu.VMEM((layers, 4, rows, each), bf16),
            pltpu.VMEM((layers, 4, rows, each), bf16),
            pltpu.VMEM((rows, cols), f32),
            pltpu.VMEM((2, rows, each), f32),
            pltpu.VMEM((layers, CONV_WIDTH, half), f32),
            pltpu.VMEM((layers, half), f32),
            pltpu.VMEM((layers, half), f32),
            pltpu.VMEM((4, layers, cols), f32),
            pltpu.VMEM((4, layers, cols), f32),
            pltpu.VMEM((layers + 1, PACK, 128), f32),
            pltpu.VMEM((layers + 1, 7, PACK, 128), f32),
            dma((3,)),
            dma((3,)), dma((18,)),
            dma((1,)), dma((units,)),
            dma((1,)), dma((6,)),
            dma((1,)), dma((13,)),
            dma((layers, 2)), dma((layers, 2)),
            dma((layers + 1,)), dma((layers + 1,)),
            dma((layers,)), dma((layers, 4)),
            dma((layers,)), dma((layers, 4)),
            dma((layers,)), dma((layers, 4)),
            dma((1,)), dma((1,)),
        ],
        compiler_params=pltpu.CompilerParams(
            collective_id=0, has_side_effects=True, vmem_limit_bytes=56 * 1024 * 1024
        ),
    )(
        tokens, pre_gain, w_value, w_gate, jnp.swapaxes(all_taps, 0, 1), norm_gain, norm_shift, w_out,
        post_gain,
    )


def solution(mesh):
    nsp, ntp = mesh.shape["sp"], mesh.shape["tp"]
    body = kernel_local if nsp == 8 and ntp == 4 else local
    placed = (
        P("sp", "tp"),
        P(),
        P(None, "sp", "tp"),
        P(None, "sp", "tp"),
        P(None, None, "tp"),
        P(None, "tp"),
        P(None, "tp"),
        P(None, "tp", "sp"),
        P(None, "tp"),
    )
    return jax.shard_map(
        body, mesh=mesh, in_specs=placed, out_specs=P("sp", "tp"), check_vma=False
    )
```

```python
import jax
import jax.numpy as jnp
from jax import lax
from jax.experimental import pallas as pl
from jax.experimental.pallas import tpu as pltpu
from jax.sharding import PartitionSpec as P

D = 2048
CONV_WIDTH = 31
LAYERS = 2


EPSILON = 1e-06
LN_EPSILON = 1e-05


def passed_along(block, axis, distance):
    devices = range(lax.axis_size(axis))
    route = [(i - distance, i) for i in devices if i - distance in devices]
    return lax.ppermute(block, axis, route)


def local(tokens, pre_gain, w_value, w_gate, taps, norm_gain, norm_shift, w_out, post_gain):
    stream = tokens
    full_value, full_gate = (
        lax.all_gather(w_value, "sp", axis=1, tiled=True),
        lax.all_gather(w_gate, "sp", axis=1, tiled=True),
    )
    full_out = lax.all_gather(w_out, "sp", axis=2, tiled=True)
    for layer in range(LAYERS):
        whole = lax.all_gather(stream, "tp", axis=1, tiled=True)
        whole_f = whole.astype(jnp.float32)
        normed = (
            whole_f
            * lax.rsqrt(jnp.mean(whole_f * whole_f, -1, keepdims=True) + EPSILON)
            * pre_gain[layer]
        ).astype(jnp.bfloat16)
        value_mat = full_value[layer]
        gate_mat = full_gate[layer]
        out_mat = full_out[layer]
        value_proj = jnp.dot(normed, value_mat, preferred_element_type=jnp.float32)
        gate_proj = jnp.dot(normed, gate_mat, preferred_element_type=jnp.float32)
        glu_act = (value_proj * jax.nn.sigmoid(gate_proj)).astype(jnp.bfloat16)
        rows = glu_act.shape[0]
        fringe = passed_along(glu_act[rows - (CONV_WIDTH - 1) :], "sp", 1)
        padded = jnp.concatenate([fringe, glu_act], 0).astype(jnp.float32)
        conv_out = jnp.zeros(glu_act.shape, jnp.float32)
        for offset in range(CONV_WIDTH):
            conv_out = conv_out + taps[layer, offset] * padded[offset : offset + rows]
        row_sum, row_square = lax.psum(
            (jnp.sum(conv_out, -1, keepdims=True), jnp.sum(conv_out * conv_out, -1, keepdims=True)),
            "tp",
        )
        center = row_sum / D
        spread = jnp.maximum(row_square / D - center * center, 0.0)
        activated = jax.nn.silu(
            (conv_out - center) * lax.rsqrt(spread + LN_EPSILON) * norm_gain[layer]
            + norm_shift[layer]
        ).astype(jnp.bfloat16)
        terms = jnp.dot(activated, out_mat, preferred_element_type=jnp.float32)
        summed = lax.psum_scatter(terms.astype(jnp.bfloat16), "tp", scatter_dimension=1, tiled=True)
        projected = summed.astype(jnp.float32)
        out_square = lax.psum(jnp.sum(projected * projected, -1, keepdims=True), "tp")
        scale = lax.rsqrt(out_square / D + EPSILON)
        stream = (stream.astype(jnp.float32) + projected * scale * post_gain[layer]).astype(
            jnp.bfloat16
        )
    return stream


TILE = 64
PACK = 16
HALO = 32
OVER_X = ((True, True), (True, False))
FAR = (1, 2, 3)
SPLIT = 3


def step(
    x_ref, pre_ref, wv_hbm, wg_hbm, taps_ref, ng_ref, ns_ref, wo_hbm, post_ref, out_ref,
    weight, other, whole, shared, stream, normed, fresh, kept, added, row_sums, row_moments, glu, conv, act,
    part_out, part_in, x_out, x_in, z_out, z_in, total, held,
    taps, gain, shift, pre_all, post_all, stat, stat_in, local_sem,
    zs, zr, ys, yr, gs, gr, fs, fr, hs, hr, ss, sr, ps, pr, xs, xr, bs, br, qs, qr,
):
    sp, tp = lax.axis_index("sp"), lax.axis_index("tp")
    rows, cols = x_ref.shape
    layers, units, nsp, ntp = 2, 6, 8, 4
    z, y = sp // 2, sp % 2
    zh, zl = z // 2, z % 2
    x, c = tp // 2, tp % 2
    plane = [z, zh * 2 + 1 - zl, (1 - zh) * 2 + zl, (1 - zh) * 2 + 1 - zl]
    partner = plane[1] * 2 + y
    beside, facing = (partner, tp), (z * 2 + 1 - y, tp)
    mate, across, diagonal = (sp, x * 2 + 1 - c), (sp, (1 - x) * 2 + c), (sp, (1 - x) * 2 + 1 - c)
    both, half, tiles = 2 * rows, cols // 2, rows // TILE
    mine = pl.ds(pl.multiple_of(zl * half, half), half)
    rest = pl.ds(pl.multiple_of((1 - zl) * half, half), half)
    depth, each = wv_hbm.shape[1], wo_hbm.shape[2]
    per = cols // each

    def copy(src, dst, send, recv, to):
        return pltpu.make_async_remote_copy(
            src_ref=src, dst_ref=dst, send_sem=send, recv_sem=recv, device_id=to,
            device_id_type=pl.DeviceIdType.MESH,
        )

    def took(b, sem):
        copy(b, b, sem, sem, mate).wait_recv()

    def left(b, sem):
        copy(b, b, sem, sem, mate).wait_send()

    def block(i, size=TILE):
        if isinstance(i, int):
            return pl.ds(i * size, size)
        return pl.ds(pl.multiple_of(i * size, size), size)

    def parts(u):
        return (0, 1) if u < SPLIT else (0,)

    def piece(u, slot):
        return weight.at[u, block(slot, depth)]

    def part_of(u, slot, part):
        if u >= SPLIT:
            return piece(u, slot)
        return weight.at[u, block(slot * 2 + part, depth // 2)]

    def landing(u, k, part):
        if u < SPLIT:
            return zr.at[(u * 3 + k - 1) * 2 + part]
        return zr.at[SPLIT * 3 + u * 3 + k - 1]

    def along(u, k, part):
        p = part_of(u, sp, part)
        src = other.at[u, block(part, depth // len(parts(u)))]
        to = (plane[k] * 2 + y, tp)
        copy(p if k == 2 else src, p, zs.at[k - 1], landing(u, k, part), to).start()

    def own(u):
        for part in parts(u):
            for k in FAR:
                along(u, k, part)

    def sideways(u, k, part=0):
        p = part_of(u, plane[k] * 2 + y, part)
        copy(p, p, ys.at[0], yr.at[u], facing).start()

    def own_sideways(u):
        for part in parts(u):
            sideways(u, 0, part)

    def relay(u, k, part):
        took(part_of(u, plane[k] * 2 + y, part), landing(u, k, part))
        sideways(u, k, part)

    def relay_near(u, part=0):
        pl.when(zl == zh)(lambda: relay(u, 2, part))
        pl.when(zl != zh)(lambda: relay(u, 3, part))

    def relay_far(u, part=0):
        pl.when(zl == zh)(lambda: relay(u, 3, part))
        pl.when(zl != zh)(lambda: relay(u, 2, part))

    def relay_beside(u, part=0):
        relay(u, 1, part)

    def relay_all(u, part=0):
        relay_near(u, part)
        relay_beside(u, part)
        relay_far(u, part)

    def arrive(u):
        took(weight.at[u, : 4 * depth], yr.at[u])

    here, there = zl * 4, (1 - zl) * 4
    opposite = (1 - x) * 2 + c
    upper, lower = pl.ds(0, rows // 2), pl.ds(rows // 2, rows // 2)
    full = pl.ds(0, rows)
    routes = dict(
        across=(here + tp, full, across, 0),
        beside_upper=(here + tp, upper, beside, 1),
        beside_lower=(here + tp, lower, beside, 2),
        mate=(here + tp, full, mate, 5),
        diagonal_upper=(there + tp, upper, across, 3),
        diagonal_lower=(there + tp, lower, across, 4),
        across_mate=(here + opposite, full, mate, 5),
        beside_mate=(there + tp, full, mate, 5),
        both_mate_upper=(there + opposite, upper, mate, 5),
        both_mate_lower=(there + opposite, lower, mate, 5),
    )

    def gather(name):
        t, part, to, k = routes[name]
        b = whole.at[t, part]
        copy(b, b, gs.at[0], gr.at[k], to).start()

    def came(name, t):
        took(whole.at[t, routes[name][1]], gr.at[routes[name][3]])

    def gather_start():
        for name in ("across", "beside_upper", "beside_lower", "mate"):
            gather(name)

    def gather_upper():
        came("beside_upper", there + tp)
        gather("diagonal_upper")

    def gather_lower():
        came("beside_lower", there + tp)
        gather("diagonal_lower")
        gather("beside_mate")

    def gather_across():
        came("across", here + opposite)
        gather("across_mate")

    def gather_last():
        came("diagonal_upper", there + opposite)
        gather("both_mate_upper")
        came("diagonal_lower", there + opposite)
        gather("both_mate_lower")

    def row_scale(square):
        return lax.rsqrt(square / (cols * ntp) + EPSILON)

    def norm():
        took(whole.at[0:4], gr.at[5])

        @pl.loop(0, 2 * tiles)
        def _(i):
            g, r = i // tiles * 4, block(i % tiles)
            square = jnp.zeros((TILE, 1), jnp.float32)
            for t in range(ntp):
                v = whole[g + t, r, :].astype(jnp.float32)
                square = square + jnp.sum(v * v, -1, keepdims=True)
            scale = row_scale(square)
            for t in range(ntp):
                v = whole[g + t, r, :].astype(jnp.float32)
                at = slice(t * cols, (t + 1) * cols)
                normed[block(i), at] = (v * scale * pre_ref[0:1, at]).astype(jnp.bfloat16)

    def project_kept(l, kind):
        w = weight[3 * l + kind]
        for part in (slice(0, rows), slice(rows, both)):
            kept[kind, part] = jnp.dot(normed[part], w, preferred_element_type=jnp.float32)

    pair_tp, pair_opposite = x * 2 + 1 - c, (1 - x) * 2 + 1 - c
    hand = dict(
        across=(here + tp, across, here + opposite, 0),
        beside=(here + tp, beside, there + tp, 2),
        diagonal=(there + tp, across, there + opposite, 4),
        across_mate=(here + opposite, mate, here + pair_opposite, 6),
        beside_mate=(there + tp, mate, there + pair_tp, 8),
        both_mate=(there + opposite, mate, there + pair_opposite, 10),
        mate=(here + tp, mate, here + pair_tp, 12),
    )

    def share(name, h):
        t, to, _, k = hand[name]
        b = shared.at[t, h]
        copy(b, b, fs.at[0], fr.at[k if name == "mate" else k + h], to).start()

    def shared_wait(name, h):
        if name == "mate":
            took(shared.at[here + pair_tp], fr.at[12])
        else:
            took(shared.at[hand[name][2], h], fr.at[hand[name][3] + h])

    def share_turn(name, h):
        shared_wait(name, h)
        if name == "beside":
            share("diagonal", h)
        share("both_mate" if name == "diagonal" else name + "_mate", h)

    def keep_old():
        @pl.loop(0, 2 * tiles)
        def _(i):
            g, r = i // tiles * 4, block(i % tiles)
            square = jnp.zeros((TILE, 128), jnp.float32)
            for t in range(ntp):
                v = whole[g + t, r, :].astype(jnp.float32)
                at = slice(t * cols, (t + 1) * cols)
                normed[block(i), at] = (v * pre_ref[1:2, at]).astype(jnp.bfloat16)
                for j in range(cols // 128):
                    w = v[:, j * 128 : (j + 1) * 128]
                    square = square + w * w
            row_sums[3, block(i), :] = square

    groups_of = dict(
        mate=(zl, x), across_mate=(zl, 1 - x), beside_mate=(1 - zl, x), both_mate=(1 - zl, 1 - x)
    )
    begun = set()

    def fold(v):
        out = v[:, :128]
        for j in range(1, each // 128):
            out = out + v[:, j * 128 : (j + 1) * 128]
        return out

    def prepare(name, h):
        q, column = groups_of[name]
        side = name in ("mate", "across_mate")
        start = ("sums", side) not in begun
        begun.add(("sums", side))
        at = slice(h * each, (h + 1) * each)

        @pl.loop(0, tiles)
        def _(i):
            r, to = block(i), block(q * tiles + i)
            sums = [jnp.zeros((TILE, 128), jnp.float32) if start else row_sums[n, to, :] for n in range(3)]
            for core in range(2):
                t = column * 2 + core
                v = shared[q * 4 + t, h, r, :].astype(jnp.float32)
                old = whole[q * 4 + t, r, at].astype(jnp.float32)
                w = v * post_all[t, 0:1, at]
                fresh[q * 4 + t, h, r, :] = (w * pre_all[t, 1:2, at]).astype(jnp.bfloat16)
                sums = [s + fold(p) for s, p in zip(sums, (v * v, old * w, w * w))]
            for n in range(3):
                row_sums[n, to, :] = sums[n]

    def multiply(name, h, kinds=(0, 1)):
        q, column = groups_of[name]
        side, to = name in ("mate", "across_mate"), block(q, rows)
        sums = []
        for kind in kinds:
            v = None
            for core in range(2):
                t = column * 2 + core
                w = weight[3 + kind, block(t * per + h, depth), :]
                p = jnp.dot(fresh[q * 4 + t, h], w, preferred_element_type=jnp.float32)
                v = p if v is None else v + p
            sums.append(v)
        for kind, v in zip(kinds, sums):
            start = (kind, side) not in begun
            begun.add((kind, side))
            added[kind, to, :] = v if start else added[kind, to, :] + v

    def scales(to):
        new, cross, square, old = [
            jnp.sum(row_sums[n, to, :], -1, keepdims=True) for n in range(4)
        ]
        s = row_scale(new)
        return s, row_scale(jnp.maximum(old + 2.0 * s * cross + s * s * square, 0.0))

    def gate_tile(l, i):
        to = block(i)
        value, gate = kept[0, to, :], kept[1, to, :]
        if l:
            s, n = scales(to)
            value = n * (value + s * added[0, to, :])
            gate = n * (gate + s * added[1, to, :])
        made = (value * jax.nn.sigmoid(gate)).astype(jnp.bfloat16)
        glu[l, i // tiles, pl.ds(HALO + i % tiles * TILE, TILE), :] = made

    def project(l):
        inner = tiles - 1
        for q in range(2):
            gate_tile(l, q * tiles + inner)
        halo_send(l, lambda h: h.start())
        for i in range(2 * inner):
            gate_tile(l, i + i // inner)

    def new_stream():
        @pl.loop(0, tiles)
        def _(i):
            r = block(i)
            s, _ = scales(block(zl * tiles + i))
            for h in range(per):
                at = slice(h * each, (h + 1) * each)
                v = shared[here + tp, h, r, :].astype(jnp.float32)
                old = whole[here + tp, r, at].astype(jnp.float32)
                stream[r, at] = (old + v * s * post_ref[0:1, at]).astype(jnp.bfloat16)

    tail, head = pl.ds(rows, HALO), pl.ds(0, HALO)

    def near_halo(l):
        return copy(glu.at[l, 0, tail], glu.at[l, y, head], hs.at[l, 0], hr.at[l, y], facing)

    def even_halo(l):
        return copy(glu.at[l, 1, tail], glu.at[l, 1, head], hs.at[l, 1], hr.at[l, 1], facing)

    def odd_halo(l):
        return copy(
            glu.at[l, 1, tail], glu.at[l, 0, head], hs.at[l, 1], hr.at[l, 0], ((z + 2) * 2, tp)
        )

    def halo_send(l, act_on):
        act_on(near_halo(l))
        pl.when(y == 0)(lambda: act_on(even_halo(l)))
        pl.when((y == 1) & (zh == 0))(lambda: act_on(odd_halo(l)))

    def halo_wait(l):
        pl.when((y == 1) | (zh == 1))(lambda: took(glu.at[l, 0, head], hr.at[l, 0]))
        took(glu.at[l, 1, head], hr.at[l, 1])

        @pl.when((y == 0) & (zh == 0))
        def _():
            glu[l, 0, :HALO] = jnp.zeros((HALO, half), jnp.bfloat16)

    peers = [mate, across, diagonal, beside]
    peers += [(partner, mate[1]), (partner, across[1]), (partner, diagonal[1])]

    def exchange(e):
        for j, to in enumerate(peers[: 3 if e == layers else 7]):
            copy(stat.at[e], stat_in.at[e, j], ss.at[e], sr.at[e], to).start()

    def inbox(e):
        return stat_in.at[e, 0 : 3 if e == layers else 7]

    def received(e):
        sums = stat[e]
        for j in range(3 if e == layers else 7):
            sums = sums + stat_in[e, j]
        return sums

    lane = lax.broadcasted_iota(jnp.int32, (PACK, 128), 1)
    groups = TILE // PACK

    def pick(sums, at):
        found = [
            jnp.sum(jnp.where(lane == at * groups + g, sums, 0.0), -1, keepdims=True)
            for g in range(groups)
        ]
        return jnp.concatenate(found, 0)

    def pack(sums, at, column):
        for g in range(groups):
            sums = jnp.where(lane == at * groups + g, column[g * PACK : (g + 1) * PACK], sums)
        return sums

    first = HALO - (CONV_WIDTH - 1)

    def convolver(l):
        def tile(q, i):
            r = pl.multiple_of(i * TILE, TILE)
            one = jnp.zeros((TILE, 128), jnp.float32)
            two = jnp.zeros((TILE, 128), jnp.float32)
            for j in range(half // 128):
                at = slice(j * 128, (j + 1) * 128)
                window = glu[l, q, pl.ds(r, TILE + HALO), at].astype(jnp.float32)
                acc = jnp.zeros((TILE, 128), jnp.float32)
                for s in range(8):
                    w = window if s == 0 else pltpu.roll(window, TILE + HALO - s, 0)
                    for k in range(CONV_WIDTH):
                        if (first + k) % 8 == s:
                            o = first + k - s
                            acc = acc + taps[l, k : k + 1, at] * w[o : o + TILE]
                conv[q, pl.ds(r, TILE), at] = acc
                one = one + acc
                two = two + acc * acc
            row_moments[0, block(q * tiles + i), :] = one
            row_moments[1, block(q * tiles + i), :] = two

        return tile

    def convolve_inner(l):
        tile, inner = convolver(l), tiles - 1
        pl.loop(0, 2 * inner)(lambda i: tile(i // inner, i % inner + 1))

    def convolve_first(l):
        tile = convolver(l)
        halo_wait(l)
        pl.loop(0, 2)(lambda q: tile(q, 0))
        sums = jnp.zeros((PACK, 128), jnp.float32)
        for i in range(2 * tiles):
            for n in range(2):
                sums = pack(sums, 2 * i + n, jnp.sum(row_moments[n, block(i), :], -1, keepdims=True))
        stat[l] = sums
        exchange(l)

    def moments(l):
        took(inbox(l), sr.at[l])

    def activate(l, q):
        sums = received(l)

        for i in range(tiles):
            at, r = q * tiles + i, block(i)
            center = pick(sums, 2 * at) / (cols * ntp)
            spread = jnp.maximum(pick(sums, 2 * at + 1) / (cols * ntp) - center * center, 0.0)
            v = (conv[q, r, :] - center) * lax.rsqrt(spread + LN_EPSILON)
            v = v * gain[l : l + 1, :] + shift[l : l + 1, :]
            act[q, r, :] = (v * jax.nn.sigmoid(v)).astype(jnp.bfloat16)

    quads = dict(D=(1 - zl, 1 - x), A=(zl, 1 - x), B=(1 - zl, x), O=(zl, x))
    names = list(quads)

    def term(l, quad, h, core):
        q, column = quads[quad]
        w = weight[3 * l + 2, block((column * 2 + core) * per + h, depth), :]
        return jnp.dot(act[q], w, preferred_element_type=jnp.float32).astype(jnp.bfloat16)

    def give(l, quad):
        i = names.index(quad)
        made = [term(l, quad, h, 1 - c) for h in range(per)]
        for h in range(per):
            part_out[l, i, h] = made[h]
        copy(part_out.at[l, i], part_in.at[l, i], ps.at[l], pr.at[l, i], mate).start()

    def joined(l, quad):
        i = names.index(quad)
        made = [term(l, quad, h, c).astype(jnp.float32) for h in range(per)]
        took(part_in.at[l, i], pr.at[l, i])
        return [made[h] + part_in[l, i, h].astype(jnp.float32) for h in range(per)]

    def pass_x(l, i, v):
        x_out[l, i] = v.astype(jnp.bfloat16)
        copy(x_out.at[l, i], x_in.at[l, i], xs.at[l], xr.at[l, i], across).start()

    def pass_z(l, i, v):
        z_out[l, i] = v.astype(jnp.bfloat16)
        copy(z_out.at[l, i], z_in.at[l, i], bs.at[l], br.at[l, i], beside).start()

    def move_on(l, quad):
        for h, v in enumerate(joined(l, quad)):
            if quad == "O":
                total[:, h * each : (h + 1) * each] = v
            elif (quad == "A" and OVER_X[l][h]) or (quad == "D" and OVER_X[l][h]):
                pass_x(l, h if quad == "D" else 2 + h, v)
            elif quad == "D" or (quad == "B" and not OVER_X[l][h]):
                pass_z(l, h if quad == "D" else 2 + h, v)
            else:
                held[h] = v

    def pass_held(l, h):
        if OVER_X[l][h]:
            took(x_in.at[l, h], xr.at[l, h])
            pass_z(l, 2 + h, held[h] + x_in[l, h].astype(jnp.float32))
        else:
            took(z_in.at[l, h], br.at[l, h])
            pass_x(l, 2 + h, held[h] + z_in[l, h].astype(jnp.float32))

    def steps(l, *todo):
        for name in todo:
            (give if name[0] == "g" else move_on)(l, name[1])

    def projected(l, h, r):
        at = slice(h * each, (h + 1) * each)
        p = total[r, at] + x_in[l, 2 + h, r, :].astype(jnp.float32)
        return (p + z_in[l, 2 + h, r, :].astype(jnp.float32)).astype(jnp.bfloat16)

    def landed(l, h):
        took(x_in.at[l, 2 + h], xr.at[l, 2 + h])
        took(z_in.at[l, 2 + h], br.at[l, 2 + h])

    def settle(h):
        landed(0, h)

        @pl.loop(0, tiles)
        def _(i):
            shared[here + tp, h, block(i), :] = projected(0, h, block(i))

        for name in ("across", "beside", "mate"):
            share(name, h)

    def finish():
        l = layers - 1
        for h in range(per):
            landed(l, h)

        def tile(i, sums):
            r = block(i)
            square = jnp.zeros((TILE, 1), jnp.float32)
            for h in range(per):
                p = projected(l, h, r).astype(jnp.float32)
                total[r, h * each : (h + 1) * each] = p
                square = square + jnp.sum(p * p, -1, keepdims=True)
            return pack(sums, i, square)

        sums = jnp.zeros((PACK, 128), jnp.float32)
        for i in range(tiles):
            sums = tile(i, sums)
        stat[layers] = sums
        exchange(layers)
        took(inbox(layers), sr.at[layers])
        sums = received(layers)
        for i in range(tiles):
            r = block(i)
            new = total[r, :] * row_scale(pick(sums, i)) * post_ref[l : l + 1, :]
            out_ref[r, :] = (stream[r, :].astype(jnp.float32) + new).astype(jnp.bfloat16)

    pltpu.make_async_copy(x_ref, whole.at[here + tp], local_sem.at[2]).start()
    for u in range(units):
        l, kind = divmod(u, 3)
        ref = (wv_hbm, wg_hbm, wo_hbm)[kind]
        for i, (part, to) in enumerate(((mine, piece(u, sp)), (rest, other.at[u]))):
            src = ref.at[l, part] if kind == 2 else ref.at[l, :, part]
            pltpu.make_async_copy(src, to, local_sem.at[i]).start()
    post_all[tp] = post_ref[...]
    for t in range(ntp):
        pre_all[t] = pre_ref[:, t * cols : (t + 1) * cols]
    for l in range(layers):
        taps[l] = taps_ref[:, l, mine]
        gain[l : l + 1] = ng_ref[l : l + 1, mine]
        shift[l : l + 1] = ns_ref[l : l + 1, mine]
    barrier = pltpu.get_barrier_semaphore()
    for i in range(1, nsp):
        pl.semaphore_signal(
            barrier, inc=1, device_id=(lax.rem(sp + i, nsp), tp),
            device_id_type=pl.DeviceIdType.MESH,
        )
    for i in range(1, ntp):
        for at in (sp, partner):
            pl.semaphore_signal(
                barrier, inc=1, device_id=(at, lax.rem(tp + i, ntp)),
                device_id_type=pl.DeviceIdType.MESH,
            )
    pl.semaphore_wait(barrier, nsp - 1 + 2 * (ntp - 1))
    for i in range(2):
        pltpu.make_async_copy(other, other, local_sem.at[i]).wait()
    pltpu.make_async_copy(x_ref, whole.at[here + tp], local_sem.at[2]).wait()

    def post_start():
        for to in (mate, across, diagonal):
            copy(post_ref, post_all.at[tp], qs.at[0], qr.at[0], to).start()

    def post_wait():
        took(post_all.at[0:3], qr.at[0])

    own(0)
    own_sideways(0)
    gather_start()
    post_start()
    own(1)
    own_sideways(1)
    own_sideways(2)
    relay_all(0)
    relay_all(0, 1)
    gather_upper()
    relay_near(1)
    gather_lower()
    relay_beside(1)
    relay_far(1)
    relay_all(1, 1)
    gather_across()
    own(2)
    own_sideways(3)
    gather_last()
    norm()
    arrive(0)
    project_kept(0, 0)
    arrive(1)
    project_kept(0, 1)
    project(0)
    relay_all(2)
    convolve_inner(0)
    convolve_first(0)
    own(3)
    own(4)
    relay_all(2, 1)
    own_sideways(4)
    moments(0)
    activate(0, 1 - zl)
    arrive(2)
    steps(0, "gD")
    activate(0, zl)
    steps(0, "gA", "mD", "gB", "mA", "gO", "mB", "mO")
    pass_held(0, 0)
    relay_near(3)
    relay_beside(3)
    pass_held(0, 1)
    relay_far(3)
    post_wait()
    keep_old()
    settle(0)
    relay_all(4)
    settle(1)
    own(5)
    own_sideways(5)
    arrive(3)
    project_kept(1, 0)
    shared_wait("mate", 0)
    prepare("mate", 0)
    prepare("mate", 1)
    share_turn("beside", 0)
    share_turn("across", 0)
    shared_wait("across_mate", 0)
    prepare("across_mate", 0)
    shared_wait("beside_mate", 0)
    prepare("beside_mate", 0)
    share_turn("beside", 1)
    share_turn("across", 1)
    arrive(4)
    project_kept(1, 1)
    share_turn("diagonal", 0)
    multiply("mate", 0)
    multiply("mate", 1)
    multiply("across_mate", 0)
    multiply("beside_mate", 0)
    shared_wait("across_mate", 1)
    prepare("across_mate", 1)
    multiply("across_mate", 1)
    shared_wait("beside_mate", 1)
    prepare("beside_mate", 1)
    multiply("beside_mate", 1)
    shared_wait("both_mate", 0)
    prepare("both_mate", 0)
    multiply("both_mate", 0)
    share_turn("diagonal", 1)
    relay_near(5)
    shared_wait("both_mate", 1)
    prepare("both_mate", 1)
    multiply("both_mate", 1)
    project(1)
    relay_beside(5)
    relay_far(5)
    convolve_inner(1)
    convolve_first(1)
    new_stream()
    moments(1)
    activate(1, 1 - zl)
    arrive(5)
    steps(1, "gD")
    activate(1, zl)
    steps(1, "gA", "mD", "gB", "mA", "gO", "mB", "mO")
    pass_held(1, 1)
    pass_held(1, 0)
    finish()
    for k in FAR:
        left(other, zs.at[k - 1])
    left(weight.at[0:3], ys.at[0])
    left(whole.at[0:7], gs.at[0])
    left(shared.at[0:7], fs.at[0])
    left(post_all.at[0:3], qs.at[0])
    for l in range(layers):
        left(inbox(l), ss.at[l])
        left(part_out.at[l], ps.at[l])
        left(x_out.at[l, 0 : 2 + sum(OVER_X[l])], xs.at[l])
        left(z_out.at[l, 0 : 4 - sum(OVER_X[l])], bs.at[l])
        halo_send(l, lambda h: h.wait_send())
    left(inbox(layers), ss.at[layers])


def kernel_local(*args):
    tokens, pre_gain, w_value, w_gate, all_taps, norm_gain, norm_shift, w_out, post_gain = args
    rows, cols = tokens.shape
    layers, depth = w_value.shape[:2]
    each = w_out.shape[2]
    half, units = cols // 2, 3 * layers
    square = depth == half == each and depth % 128 == 0
    if rows % TILE or 4 * rows > PACK * 128 or layers != 2 or not square:
        return local(*args)
    vmem, hbm = pl.BlockSpec(memory_space=pltpu.VMEM), pl.BlockSpec(memory_space=pl.ANY)
    bf16, f32, dma = jnp.bfloat16, jnp.float32, pltpu.SemaphoreType.DMA
    return pl.pallas_call(
        step,
        out_shape=pltpu.VMEM((rows, cols), bf16),
        in_specs=[hbm, vmem, hbm, hbm, vmem, vmem, vmem, hbm, vmem],
        out_specs=vmem,
        scratch_shapes=[
            pltpu.VMEM((units, 8 * depth, half), bf16),
            pltpu.VMEM((units, depth, half), bf16),
            pltpu.VMEM((8, rows, cols), bf16),
            pltpu.VMEM((8, 2, rows, each), bf16),
            pltpu.VMEM((rows, cols), bf16),
            pltpu.VMEM((2 * rows, 4 * cols), bf16),
            pltpu.VMEM((8, 2, rows, each), bf16),
            pltpu.VMEM((2, 2 * rows, half), f32),
            pltpu.VMEM((2, 2 * rows, half), f32),
            pltpu.VMEM((4, 2 * rows, 128), f32),
            pltpu.VMEM((2, 2 * rows, 128), f32),
            pltpu.VMEM((layers, 2, HALO + rows, half), bf16),
            pltpu.VMEM((2, rows, half), f32),
            pltpu.VMEM((2, rows, half), bf16),
            pltpu.VMEM((layers, 4, 2, rows, each), bf16),
            pltpu.VMEM((layers, 4, 2, rows, each), bf16),
            pltpu.VMEM((layers, 4, rows, each), bf16),
            pltpu.VMEM((layers, 4, rows, each), bf16),
            pltpu.VMEM((layers, 4, rows, each), bf16),
            pltpu.VMEM((layers, 4, rows, each), bf16),
            pltpu.VMEM((rows, cols), f32),
            pltpu.VMEM((2, rows, each), f32),
            pltpu.VMEM((layers, CONV_WIDTH, half), f32),
            pltpu.VMEM((layers, half), f32),
            pltpu.VMEM((layers, half), f32),
            pltpu.VMEM((4, layers, cols), f32),
            pltpu.VMEM((4, layers, cols), f32),
            pltpu.VMEM((layers + 1, PACK, 128), f32),
            pltpu.VMEM((layers + 1, 7, PACK, 128), f32),
            dma((3,)),
            dma((3,)), dma((18 + 3 * SPLIT,)),
            dma((1,)), dma((units,)),
            dma((1,)), dma((6,)),
            dma((1,)), dma((13,)),
            dma((layers, 2)), dma((layers, 2)),
            dma((layers + 1,)), dma((layers + 1,)),
            dma((layers,)), dma((layers, 4)),
            dma((layers,)), dma((layers, 4)),
            dma((layers,)), dma((layers, 4)),
            dma((1,)), dma((1,)),
        ],
        compiler_params=pltpu.CompilerParams(
            collective_id=0, has_side_effects=True, vmem_limit_bytes=56 * 1024 * 1024
        ),
    )(
        tokens, pre_gain, w_value, w_gate, jnp.swapaxes(all_taps, 0, 1), norm_gain, norm_shift, w_out,
        post_gain,
    )


def solution(mesh):
    nsp, ntp = mesh.shape["sp"], mesh.shape["tp"]
    body = kernel_local if nsp == 8 and ntp == 4 else local
    placed = (
        P("sp", "tp"),
        P(),
        P(None, "sp", "tp"),
        P(None, "sp", "tp"),
        P(None, None, "tp"),
        P(None, "tp"),
        P(None, "tp"),
        P(None, "tp", "sp"),
        P(None, "tp"),
    )
    return jax.shard_map(
        body, mesh=mesh, in_specs=placed, out_specs=P("sp", "tp"), check_vma=False
    )
```

```python
import jax
import jax.numpy as jnp
from jax import lax
from jax.experimental import pallas as pl
from jax.experimental.pallas import tpu as pltpu
from jax.sharding import PartitionSpec as P

D = 2048
CONV_WIDTH = 31
LAYERS = 2


EPSILON = 1e-06
LN_EPSILON = 1e-05


def passed_along(block, axis, distance):
    devices = range(lax.axis_size(axis))
    route = [(i - distance, i) for i in devices if i - distance in devices]
    return lax.ppermute(block, axis, route)


def local(tokens, pre_gain, w_value, w_gate, taps, norm_gain, norm_shift, w_out, post_gain):
    stream = tokens
    full_value, full_gate = (
        lax.all_gather(w_value, "sp", axis=1, tiled=True),
        lax.all_gather(w_gate, "sp", axis=1, tiled=True),
    )
    full_out = lax.all_gather(w_out, "sp", axis=2, tiled=True)
    for layer in range(LAYERS):
        whole = lax.all_gather(stream, "tp", axis=1, tiled=True)
        whole_f = whole.astype(jnp.float32)
        normed = (
            whole_f
            * lax.rsqrt(jnp.mean(whole_f * whole_f, -1, keepdims=True) + EPSILON)
            * pre_gain[layer]
        ).astype(jnp.bfloat16)
        value_mat = full_value[layer]
        gate_mat = full_gate[layer]
        out_mat = full_out[layer]
        value_proj = jnp.dot(normed, value_mat, preferred_element_type=jnp.float32)
        gate_proj = jnp.dot(normed, gate_mat, preferred_element_type=jnp.float32)
        glu_act = (value_proj * jax.nn.sigmoid(gate_proj)).astype(jnp.bfloat16)
        rows = glu_act.shape[0]
        fringe = passed_along(glu_act[rows - (CONV_WIDTH - 1) :], "sp", 1)
        padded = jnp.concatenate([fringe, glu_act], 0).astype(jnp.float32)
        conv_out = jnp.zeros(glu_act.shape, jnp.float32)
        for offset in range(CONV_WIDTH):
            conv_out = conv_out + taps[layer, offset] * padded[offset : offset + rows]
        row_sum, row_square = lax.psum(
            (jnp.sum(conv_out, -1, keepdims=True), jnp.sum(conv_out * conv_out, -1, keepdims=True)),
            "tp",
        )
        center = row_sum / D
        spread = jnp.maximum(row_square / D - center * center, 0.0)
        activated = jax.nn.silu(
            (conv_out - center) * lax.rsqrt(spread + LN_EPSILON) * norm_gain[layer]
            + norm_shift[layer]
        ).astype(jnp.bfloat16)
        terms = jnp.dot(activated, out_mat, preferred_element_type=jnp.float32)
        summed = lax.psum_scatter(terms.astype(jnp.bfloat16), "tp", scatter_dimension=1, tiled=True)
        projected = summed.astype(jnp.float32)
        out_square = lax.psum(jnp.sum(projected * projected, -1, keepdims=True), "tp")
        scale = lax.rsqrt(out_square / D + EPSILON)
        stream = (stream.astype(jnp.float32) + projected * scale * post_gain[layer]).astype(
            jnp.bfloat16
        )
    return stream


TILE = 64
PACK = 16
HALO = 32
OVER_X = ((True, True), (True, False))
FAR = (1, 2, 3)
PARTS = (2, 2, 4, 1, 1, 2)


def step(
    x_ref, pre_hbm, wv_hbm, wg_hbm, taps_hbm, ng_hbm, ns_hbm, wo_hbm, post_hbm, out_ref,
    pre_ref, taps_ref, ng_ref, ns_ref, post_ref,
    weight, other, whole, shared, stream, normed, fresh, kept, added, row_sums, row_moments, glu, conv, act,
    part_out, part_in, x_out, x_in, z_out, z_in, total, held,
    taps, gain, shift, pre_all, post_all, stat, stat_in, local_sem,
    zs, zr, ys, yr, gs, gr, fs, fr, hs, hr, ss, sr, ps, pr, xs, xr, bs, br, qs, qr,
):
    sp, tp = lax.axis_index("sp"), lax.axis_index("tp")
    rows, cols = x_ref.shape
    layers, units, nsp, ntp = 2, 6, 8, 4
    z, y = sp // 2, sp % 2
    zh, zl = z // 2, z % 2
    x, c = tp // 2, tp % 2
    plane = [z, zh * 2 + 1 - zl, (1 - zh) * 2 + zl, (1 - zh) * 2 + 1 - zl]
    partner = plane[1] * 2 + y
    beside, facing = (partner, tp), (z * 2 + 1 - y, tp)
    mate, across, diagonal = (sp, x * 2 + 1 - c), (sp, (1 - x) * 2 + c), (sp, (1 - x) * 2 + 1 - c)
    both, half, tiles = 2 * rows, cols // 2, rows // TILE
    mine = pl.ds(pl.multiple_of(zl * half, half), half)
    rest = pl.ds(pl.multiple_of((1 - zl) * half, half), half)
    depth, each = wv_hbm.shape[1], wo_hbm.shape[2]
    per = cols // each

    def copy(src, dst, send, recv, to):
        return pltpu.make_async_remote_copy(
            src_ref=src, dst_ref=dst, send_sem=send, recv_sem=recv, device_id=to,
            device_id_type=pl.DeviceIdType.MESH,
        )

    def took(b, sem):
        copy(b, b, sem, sem, mate).wait_recv()

    def left(b, sem):
        copy(b, b, sem, sem, mate).wait_send()

    def block(i, size=TILE):
        if isinstance(i, int):
            return pl.ds(i * size, size)
        return pl.ds(pl.multiple_of(i * size, size), size)

    def parts(u):
        return range(PARTS[u])

    def piece(u, slot):
        return weight.at[u, block(slot, depth)]

    def part_of(u, slot, part):
        return weight.at[u, block(slot * PARTS[u] + part, depth // PARTS[u])]

    def landing(u, k, part):
        return zr.at[3 * (sum(PARTS[:u]) + part) + k - 1]

    def along(u, k, part):
        p = part_of(u, sp, part)
        src = other.at[u, block(part, depth // PARTS[u])]
        to = (plane[k] * 2 + y, tp)
        copy(p if k == 2 else src, p, zs.at[k - 1], landing(u, k, part), to).start()

    def own(u, *some):
        for part in some or parts(u):
            for k in FAR:
                along(u, k, part)

    def sideways(u, k, part=0):
        p = part_of(u, plane[k] * 2 + y, part)
        copy(p, p, ys.at[0], yr.at[u], facing).start()

    def own_sideways(u):
        for part in parts(u):
            sideways(u, 0, part)

    def relay(u, k, part):
        took(part_of(u, plane[k] * 2 + y, part), landing(u, k, part))
        sideways(u, k, part)

    def relay_near(u, part=0):
        pl.when(zl == zh)(lambda: relay(u, 2, part))
        pl.when(zl != zh)(lambda: relay(u, 3, part))

    def relay_far(u, part=0):
        pl.when(zl == zh)(lambda: relay(u, 3, part))
        pl.when(zl != zh)(lambda: relay(u, 2, part))

    def relay_beside(u, part=0):
        relay(u, 1, part)

    def relay_all(u, *some):
        for part in some or (0,):
            relay_near(u, part)
            relay_beside(u, part)
            relay_far(u, part)

    def arrive(u):
        took(weight.at[u, : 4 * depth], yr.at[u])

    here, there = zl * 4, (1 - zl) * 4
    opposite = (1 - x) * 2 + c
    upper, lower = pl.ds(0, rows // 2), pl.ds(rows // 2, rows // 2)
    full = pl.ds(0, rows)
    routes = dict(
        across=(here + tp, full, across, 0),
        beside_upper=(here + tp, upper, beside, 1),
        beside_lower=(here + tp, lower, beside, 2),
        mate=(here + tp, full, mate, 5),
        diagonal_upper=(there + tp, upper, across, 3),
        diagonal_lower=(there + tp, lower, across, 4),
        across_mate=(here + opposite, full, mate, 5),
        beside_mate=(there + tp, full, mate, 5),
        both_mate_upper=(there + opposite, upper, mate, 5),
        both_mate_lower=(there + opposite, lower, mate, 5),
    )

    def gather(name):
        t, part, to, k = routes[name]
        b = whole.at[t, part]
        copy(b, b, gs.at[0], gr.at[k], to).start()

    def came(name, t):
        took(whole.at[t, routes[name][1]], gr.at[routes[name][3]])

    def gather_start():
        for name in ("across", "beside_upper", "beside_lower", "mate"):
            gather(name)

    def gather_upper():
        came("beside_upper", there + tp)
        gather("diagonal_upper")

    def gather_lower():
        came("beside_lower", there + tp)
        gather("diagonal_lower")
        gather("beside_mate")

    def gather_across():
        came("across", here + opposite)
        gather("across_mate")

    def gather_last():
        came("diagonal_upper", there + opposite)
        gather("both_mate_upper")
        came("diagonal_lower", there + opposite)
        gather("both_mate_lower")

    def row_scale(square):
        return lax.rsqrt(square / (cols * ntp) + EPSILON)

    def norm():
        took(whole.at[0:4], gr.at[5])

        @pl.loop(0, 2 * tiles)
        def _(i):
            g, r = i // tiles * 4, block(i % tiles)
            square = jnp.zeros((TILE, 1), jnp.float32)
            for t in range(ntp):
                v = whole[g + t, r, :].astype(jnp.float32)
                square = square + jnp.sum(v * v, -1, keepdims=True)
            scale = row_scale(square)
            for t in range(ntp):
                v = whole[g + t, r, :].astype(jnp.float32)
                at = slice(t * cols, (t + 1) * cols)
                normed[block(i), at] = (v * scale * pre_ref[0:1, at]).astype(jnp.bfloat16)

    def project_kept(l, kind):
        w = weight[3 * l + kind]
        for part in (slice(0, rows), slice(rows, both)):
            kept[kind, part] = jnp.dot(normed[part], w, preferred_element_type=jnp.float32)

    pair_tp, pair_opposite = x * 2 + 1 - c, (1 - x) * 2 + 1 - c
    hand = dict(
        across=(here + tp, across, here + opposite, 0),
        beside=(here + tp, beside, there + tp, 2),
        diagonal=(there + tp, across, there + opposite, 4),
        across_mate=(here + opposite, mate, here + pair_opposite, 6),
        beside_mate=(there + tp, mate, there + pair_tp, 8),
        both_mate=(there + opposite, mate, there + pair_opposite, 10),
        mate=(here + tp, mate, here + pair_tp, 12),
    )

    def share(name, h):
        t, to, _, k = hand[name]
        b = shared.at[t, h]
        copy(b, b, fs.at[0], fr.at[k if name == "mate" else k + h], to).start()

    def shared_wait(name, h):
        if name == "mate":
            took(shared.at[here + pair_tp], fr.at[12])
        else:
            took(shared.at[hand[name][2], h], fr.at[hand[name][3] + h])

    def share_turn(name, h):
        shared_wait(name, h)
        if name == "beside":
            share("diagonal", h)
        share("both_mate" if name == "diagonal" else name + "_mate", h)

    def keep_old():
        @pl.loop(0, 2 * tiles)
        def _(i):
            g, r = i // tiles * 4, block(i % tiles)
            square = jnp.zeros((TILE, 128), jnp.float32)
            for t in range(ntp):
                v = whole[g + t, r, :].astype(jnp.float32)
                at = slice(t * cols, (t + 1) * cols)
                normed[block(i), at] = (v * pre_ref[1:2, at]).astype(jnp.bfloat16)
                for j in range(cols // 128):
                    w = v[:, j * 128 : (j + 1) * 128]
                    square = square + w * w
            row_sums[3, block(i), :] = square

    groups_of = dict(
        mate=(zl, x), across_mate=(zl, 1 - x), beside_mate=(1 - zl, x), both_mate=(1 - zl, 1 - x)
    )
    begun = set()

    def fold(v):
        out = v[:, :128]
        for j in range(1, each // 128):
            out = out + v[:, j * 128 : (j + 1) * 128]
        return out

    def prepare(name, h):
        q, column = groups_of[name]
        side = name in ("mate", "across_mate")
        start = ("sums", side) not in begun
        begun.add(("sums", side))
        at = slice(h * each, (h + 1) * each)

        @pl.loop(0, tiles)
        def _(i):
            r, to = block(i), block(q * tiles + i)
            sums = [jnp.zeros((TILE, 128), jnp.float32) if start else row_sums[n, to, :] for n in range(3)]
            for core in range(2):
                t = column * 2 + core
                v = shared[q * 4 + t, h, r, :].astype(jnp.float32)
                old = whole[q * 4 + t, r, at].astype(jnp.float32)
                w = v * post_all[t, 0:1, at]
                fresh[q * 4 + t, h, r, :] = (w * pre_all[t, 1:2, at]).astype(jnp.bfloat16)
                sums = [s + fold(p) for s, p in zip(sums, (v * v, old * w, w * w))]
            for n in range(3):
                row_sums[n, to, :] = sums[n]

    def multiply(name, h, kinds=(0, 1)):
        q, column = groups_of[name]
        side, to = name in ("mate", "across_mate"), block(q, rows)
        sums = []
        for kind in kinds:
            v = None
            for core in range(2):
                t = column * 2 + core
                w = weight[3 + kind, block(t * per + h, depth), :]
                p = jnp.dot(fresh[q * 4 + t, h], w, preferred_element_type=jnp.float32)
                v = p if v is None else v + p
            sums.append(v)
        for kind, v in zip(kinds, sums):
            start = (kind, side) not in begun
            begun.add((kind, side))
            added[kind, to, :] = v if start else added[kind, to, :] + v

    def scales(to):
        new, cross, square, old = [
            jnp.sum(row_sums[n, to, :], -1, keepdims=True) for n in range(4)
        ]
        s = row_scale(new)
        return s, row_scale(jnp.maximum(old + 2.0 * s * cross + s * s * square, 0.0))

    def gate_tile(l, i):
        to = block(i)
        value, gate = kept[0, to, :], kept[1, to, :]
        if l:
            s, n = scales(to)
            value = n * (value + s * added[0, to, :])
            gate = n * (gate + s * added[1, to, :])
        made = (value * jax.nn.sigmoid(gate)).astype(jnp.bfloat16)
        glu[l, i // tiles, pl.ds(HALO + i % tiles * TILE, TILE), :] = made

    def project(l):
        inner = tiles - 1
        for q in range(2):
            gate_tile(l, q * tiles + inner)
        halo_send(l, lambda h: h.start())
        for i in range(2 * inner):
            gate_tile(l, i + i // inner)

    def new_stream():
        @pl.loop(0, tiles)
        def _(i):
            r = block(i)
            s, _ = scales(block(zl * tiles + i))
            for h in range(per):
                at = slice(h * each, (h + 1) * each)
                v = shared[here + tp, h, r, :].astype(jnp.float32)
                old = whole[here + tp, r, at].astype(jnp.float32)
                stream[r, at] = (old + v * s * post_ref[0:1, at]).astype(jnp.bfloat16)

    tail, head = pl.ds(rows, HALO), pl.ds(0, HALO)

    def near_halo(l):
        return copy(glu.at[l, 0, tail], glu.at[l, y, head], hs.at[l, 0], hr.at[l, y], facing)

    def even_halo(l):
        return copy(glu.at[l, 1, tail], glu.at[l, 1, head], hs.at[l, 1], hr.at[l, 1], facing)

    def odd_halo(l):
        return copy(
            glu.at[l, 1, tail], glu.at[l, 0, head], hs.at[l, 1], hr.at[l, 0], ((z + 2) * 2, tp)
        )

    def halo_send(l, act_on):
        act_on(near_halo(l))
        pl.when(y == 0)(lambda: act_on(even_halo(l)))
        pl.when((y == 1) & (zh == 0))(lambda: act_on(odd_halo(l)))

    def halo_wait(l):
        pl.when((y == 1) | (zh == 1))(lambda: took(glu.at[l, 0, head], hr.at[l, 0]))
        took(glu.at[l, 1, head], hr.at[l, 1])

        @pl.when((y == 0) & (zh == 0))
        def _():
            glu[l, 0, :HALO] = jnp.zeros((HALO, half), jnp.bfloat16)

    peers = [mate, across, diagonal, beside]
    peers += [(partner, mate[1]), (partner, across[1]), (partner, diagonal[1])]

    def exchange(e):
        for j, to in enumerate(peers[: 3 if e == layers else 7]):
            copy(stat.at[e], stat_in.at[e, j], ss.at[e], sr.at[e], to).start()

    def inbox(e):
        return stat_in.at[e, 0 : 3 if e == layers else 7]

    def received(e):
        sums = stat[e]
        for j in range(3 if e == layers else 7):
            sums = sums + stat_in[e, j]
        return sums

    lane = lax.broadcasted_iota(jnp.int32, (PACK, 128), 1)
    groups = TILE // PACK

    def pick(sums, at):
        found = [
            jnp.sum(jnp.where(lane == at * groups + g, sums, 0.0), -1, keepdims=True)
            for g in range(groups)
        ]
        return jnp.concatenate(found, 0)

    def pack(sums, at, column):
        for g in range(groups):
            sums = jnp.where(lane == at * groups + g, column[g * PACK : (g + 1) * PACK], sums)
        return sums

    first = HALO - (CONV_WIDTH - 1)

    def convolver(l):
        def tile(q, i):
            r = pl.multiple_of(i * TILE, TILE)
            one = jnp.zeros((TILE, 128), jnp.float32)
            two = jnp.zeros((TILE, 128), jnp.float32)
            for j in range(half // 128):
                at = slice(j * 128, (j + 1) * 128)
                window = glu[l, q, pl.ds(r, TILE + HALO), at].astype(jnp.float32)
                acc = jnp.zeros((TILE, 128), jnp.float32)
                for s in range(8):
                    w = window if s == 0 else pltpu.roll(window, TILE + HALO - s, 0)
                    for k in range(CONV_WIDTH):
                        if (first + k) % 8 == s:
                            o = first + k - s
                            acc = acc + taps[l, k : k + 1, at] * w[o : o + TILE]
                conv[q, pl.ds(r, TILE), at] = acc
                one = one + acc
                two = two + acc * acc
            row_moments[0, block(q * tiles + i), :] = one
            row_moments[1, block(q * tiles + i), :] = two

        return tile

    def convolve_inner(l):
        tile, inner = convolver(l), tiles - 1
        pl.loop(0, 2 * inner)(lambda i: tile(i // inner, i % inner + 1))

    def convolve_first(l):
        tile = convolver(l)
        halo_wait(l)
        pl.loop(0, 2)(lambda q: tile(q, 0))
        sums = jnp.zeros((PACK, 128), jnp.float32)
        for i in range(2 * tiles):
            for n in range(2):
                sums = pack(sums, 2 * i + n, jnp.sum(row_moments[n, block(i), :], -1, keepdims=True))
        stat[l] = sums
        exchange(l)

    def moments(l):
        took(inbox(l), sr.at[l])

    def activate(l, q):
        sums = received(l)

        for i in range(tiles):
            at, r = q * tiles + i, block(i)
            center = pick(sums, 2 * at) / (cols * ntp)
            spread = jnp.maximum(pick(sums, 2 * at + 1) / (cols * ntp) - center * center, 0.0)
            v = (conv[q, r, :] - center) * lax.rsqrt(spread + LN_EPSILON)
            v = v * gain[l : l + 1, :] + shift[l : l + 1, :]
            act[q, r, :] = (v * jax.nn.sigmoid(v)).astype(jnp.bfloat16)

    quads = dict(D=(1 - zl, 1 - x), A=(zl, 1 - x), B=(1 - zl, x), O=(zl, x))
    names = list(quads)

    def term(l, quad, h, core):
        q, column = quads[quad]
        w = weight[3 * l + 2, block((column * 2 + core) * per + h, depth), :]
        return jnp.dot(act[q], w, preferred_element_type=jnp.float32).astype(jnp.bfloat16)

    def give(l, quad):
        i = names.index(quad)
        made = [term(l, quad, h, 1 - c) for h in range(per)]
        for h in range(per):
            part_out[l, i, h] = made[h]
        copy(part_out.at[l, i], part_in.at[l, i], ps.at[l], pr.at[l, i], mate).start()

    def joined(l, quad):
        i = names.index(quad)
        made = [term(l, quad, h, c).astype(jnp.float32) for h in range(per)]
        took(part_in.at[l, i], pr.at[l, i])
        return [made[h] + part_in[l, i, h].astype(jnp.float32) for h in range(per)]

    def pass_x(l, i, v):
        x_out[l, i] = v.astype(jnp.bfloat16)
        copy(x_out.at[l, i], x_in.at[l, i], xs.at[l], xr.at[l, i], across).start()

    def pass_z(l, i, v):
        z_out[l, i] = v.astype(jnp.bfloat16)
        copy(z_out.at[l, i], z_in.at[l, i], bs.at[l], br.at[l, i], beside).start()

    def move_on(l, quad):
        for h, v in enumerate(joined(l, quad)):
            if quad == "O":
                total[:, h * each : (h + 1) * each] = v
            elif (quad == "A" and OVER_X[l][h]) or (quad == "D" and OVER_X[l][h]):
                pass_x(l, h if quad == "D" else 2 + h, v)
            elif quad == "D" or (quad == "B" and not OVER_X[l][h]):
                pass_z(l, h if quad == "D" else 2 + h, v)
            else:
                held[h] = v

    def pass_held(l, h):
        if OVER_X[l][h]:
            took(x_in.at[l, h], xr.at[l, h])
            pass_z(l, 2 + h, held[h] + x_in[l, h].astype(jnp.float32))
        else:
            took(z_in.at[l, h], br.at[l, h])
            pass_x(l, 2 + h, held[h] + z_in[l, h].astype(jnp.float32))

    def steps(l, *todo):
        for name in todo:
            (give if name[0] == "g" else move_on)(l, name[1])

    def projected(l, h, r):
        at = slice(h * each, (h + 1) * each)
        p = total[r, at] + x_in[l, 2 + h, r, :].astype(jnp.float32)
        return (p + z_in[l, 2 + h, r, :].astype(jnp.float32)).astype(jnp.bfloat16)

    def landed(l, h):
        took(x_in.at[l, 2 + h], xr.at[l, 2 + h])
        took(z_in.at[l, 2 + h], br.at[l, 2 + h])

    def settle(h):
        landed(0, h)

        @pl.loop(0, tiles)
        def _(i):
            shared[here + tp, h, block(i), :] = projected(0, h, block(i))

        for name in ("across", "beside", "mate"):
            share(name, h)

    def finish():
        l = layers - 1
        for h in range(per):
            landed(l, h)

        def tile(i, sums):
            r = block(i)
            square = jnp.zeros((TILE, 1), jnp.float32)
            for h in range(per):
                p = projected(l, h, r).astype(jnp.float32)
                total[r, h * each : (h + 1) * each] = p
                square = square + jnp.sum(p * p, -1, keepdims=True)
            return pack(sums, i, square)

        sums = jnp.zeros((PACK, 128), jnp.float32)
        for i in range(tiles):
            sums = tile(i, sums)
        stat[layers] = sums
        exchange(layers)
        took(inbox(layers), sr.at[layers])
        sums = received(layers)
        for i in range(tiles):
            r = block(i)
            new = total[r, :] * row_scale(pick(sums, i)) * post_ref[l : l + 1, :]
            out_ref[r, :] = (stream[r, :].astype(jnp.float32) + new).astype(jnp.bfloat16)

    barrier = pltpu.get_barrier_semaphore()
    for i in range(1, nsp):
        pl.semaphore_signal(
            barrier, inc=1, device_id=(lax.rem(sp + i, nsp), tp),
            device_id_type=pl.DeviceIdType.MESH,
        )
    for i in range(1, ntp):
        for at in (sp, partner):
            pl.semaphore_signal(
                barrier, inc=1, device_id=(at, lax.rem(tp + i, ntp)),
                device_id_type=pl.DeviceIdType.MESH,
            )
    small = [
        pltpu.make_async_copy(src, dst, local_sem.at[units + 1 + i])
        for i, (src, dst) in enumerate((
            (post_hbm, post_ref), (pre_hbm, pre_ref), (taps_hbm, taps_ref), (ng_hbm, ng_ref),
            (ns_hbm, ns_ref),
        ))
    ]
    tokens = pltpu.make_async_copy(x_ref, whole.at[here + tp], local_sem.at[units])
    for u in range(units):
        l, kind = divmod(u, 3)
        ref = (wv_hbm, wg_hbm, wo_hbm)[kind]
        for part, to in ((rest, other.at[u]), (mine, piece(u, sp))):
            src = ref.at[l, part] if kind == 2 else ref.at[l, :, part]
            pltpu.make_async_copy(src, to, local_sem.at[u]).start()
        if u == 0:
            tokens.start()
            small[0].start()
    for s in small[1:]:
        s.start()
    pl.semaphore_wait(barrier, nsp - 1 + 2 * (ntp - 1))

    def fetched(u):
        pltpu.make_async_copy(other.at[0:2], other.at[0:2], local_sem.at[u]).wait()

    def set_up():
        for s in small[1:]:
            s.wait()
        for t in range(ntp):
            pre_all[t] = pre_ref[:, t * cols : (t + 1) * cols]
        for l in range(layers):
            taps[l] = taps_ref[:, l, mine]
            gain[l : l + 1] = ng_ref[l : l + 1, mine]
            shift[l : l + 1] = ns_ref[l : l + 1, mine]

    def post_start():
        small[0].wait()
        post_all[tp] = post_ref[...]
        for to in (mate, across, diagonal):
            copy(post_ref, post_all.at[tp], qs.at[0], qr.at[0], to).start()

    def post_wait():
        took(post_all.at[0:3], qr.at[0])

    fetched(0)
    own(0)
    own_sideways(0)
    tokens.wait()
    gather_start()
    fetched(1)
    own(1)
    own_sideways(1)
    fetched(2)
    own_sideways(2)
    post_start()
    set_up()
    for u in range(3, units):
        fetched(u)
    relay_all(0)
    relay_all(0, 1)
    gather_upper()
    relay_near(1)
    gather_lower()
    relay_beside(1)
    relay_far(1)
    relay_all(1, 1)
    gather_across()
    own(2, 0, 1, 2)
    own_sideways(3)
    gather_last()
    norm()
    arrive(0)
    project_kept(0, 0)
    arrive(1)
    project_kept(0, 1)
    project(0)
    own(2, 3)
    relay_all(2, 0, 1)
    convolve_inner(0)
    relay_all(2, 2)
    convolve_first(0)
    own(3)
    own(4)
    relay_all(2, 3)
    own_sideways(4)
    moments(0)
    activate(0, 1 - zl)
    activate(0, zl)
    arrive(2)
    steps(0, "gD", "gA", "mD", "gB", "mA", "gO", "mB", "mO")
    pass_held(0, 0)
    pass_held(0, 1)
    relay_all(3)
    post_wait()
    keep_old()
    settle(0)
    relay_all(4)
    settle(1)
    own_sideways(5)
    arrive(3)
    project_kept(1, 0)
    shared_wait("mate", 0)
    prepare("mate", 0)
    prepare("mate", 1)
    share_turn("beside", 0)
    own(5, 0)
    share_turn("across", 0)
    shared_wait("across_mate", 0)
    prepare("across_mate", 0)
    shared_wait("beside_mate", 0)
    prepare("beside_mate", 0)
    share_turn("beside", 1)
    own(5, 1)
    share_turn("across", 1)
    arrive(4)
    project_kept(1, 1)
    share_turn("diagonal", 0)
    multiply("mate", 0)
    multiply("mate", 1)
    multiply("across_mate", 0)
    multiply("beside_mate", 0)
    shared_wait("across_mate", 1)
    prepare("across_mate", 1)
    multiply("across_mate", 1)
    shared_wait("beside_mate", 1)
    prepare("beside_mate", 1)
    multiply("beside_mate", 1)
    shared_wait("both_mate", 0)
    prepare("both_mate", 0)
    multiply("both_mate", 0)
    share_turn("diagonal", 1)
    relay_all(5)
    shared_wait("both_mate", 1)
    prepare("both_mate", 1)
    multiply("both_mate", 1)
    project(1)
    convolve_inner(1)
    relay_all(5, 1)
    convolve_first(1)
    new_stream()
    moments(1)
    activate(1, 1 - zl)
    activate(1, zl)
    arrive(5)
    steps(1, "gD", "gA", "mD", "gB", "mA", "gO", "mB", "mO")
    pass_held(1, 1)
    pass_held(1, 0)
    finish()
    for k in FAR:
        left(other, zs.at[k - 1])
    left(weight.at[0:3], ys.at[0])
    left(whole.at[0:7], gs.at[0])
    left(shared.at[0:7], fs.at[0])
    left(post_all.at[0:3], qs.at[0])
    for l in range(layers):
        left(inbox(l), ss.at[l])
        left(part_out.at[l], ps.at[l])
        left(x_out.at[l, 0 : 2 + sum(OVER_X[l])], xs.at[l])
        left(z_out.at[l, 0 : 4 - sum(OVER_X[l])], bs.at[l])
        halo_send(l, lambda h: h.wait_send())
    left(inbox(layers), ss.at[layers])


def kernel_local(*args):
    tokens, pre_gain, w_value, w_gate, all_taps, norm_gain, norm_shift, w_out, post_gain = args
    rows, cols = tokens.shape
    layers, depth = w_value.shape[:2]
    each = w_out.shape[2]
    half, units = cols // 2, 3 * layers
    square = depth == half == each and depth % 128 == 0
    if rows % TILE or 4 * rows > PACK * 128 or layers != 2 or not square:
        return local(*args)
    vmem, hbm = pl.BlockSpec(memory_space=pltpu.VMEM), pl.BlockSpec(memory_space=pl.ANY)
    bf16, f32, dma = jnp.bfloat16, jnp.float32, pltpu.SemaphoreType.DMA
    return pl.pallas_call(
        step,
        out_shape=pltpu.VMEM((rows, cols), bf16),
        in_specs=[hbm] * 9,
        out_specs=vmem,
        scratch_shapes=[
            pltpu.VMEM((layers, 4 * cols), f32),
            pltpu.VMEM((CONV_WIDTH, layers, cols), f32),
            pltpu.VMEM((layers, cols), f32),
            pltpu.VMEM((layers, cols), f32),
            pltpu.VMEM((layers, cols), f32),
            pltpu.VMEM((units, 8 * depth, half), bf16),
            pltpu.VMEM((units, depth, half), bf16),
            pltpu.VMEM((8, rows, cols), bf16),
            pltpu.VMEM((8, 2, rows, each), bf16),
            pltpu.VMEM((rows, cols), bf16),
            pltpu.VMEM((2 * rows, 4 * cols), bf16),
            pltpu.VMEM((8, 2, rows, each), bf16),
            pltpu.VMEM((2, 2 * rows, half), f32),
            pltpu.VMEM((2, 2 * rows, half), f32),
            pltpu.VMEM((4, 2 * rows, 128), f32),
            pltpu.VMEM((2, 2 * rows, 128), f32),
            pltpu.VMEM((layers, 2, HALO + rows, half), bf16),
            pltpu.VMEM((2, rows, half), f32),
            pltpu.VMEM((2, rows, half), bf16),
            pltpu.VMEM((layers, 4, 2, rows, each), bf16),
            pltpu.VMEM((layers, 4, 2, rows, each), bf16),
            pltpu.VMEM((layers, 4, rows, each), bf16),
            pltpu.VMEM((layers, 4, rows, each), bf16),
            pltpu.VMEM((layers, 4, rows, each), bf16),
            pltpu.VMEM((layers, 4, rows, each), bf16),
            pltpu.VMEM((rows, cols), f32),
            pltpu.VMEM((2, rows, each), f32),
            pltpu.VMEM((layers, CONV_WIDTH, half), f32),
            pltpu.VMEM((layers, half), f32),
            pltpu.VMEM((layers, half), f32),
            pltpu.VMEM((4, layers, cols), f32),
            pltpu.VMEM((4, layers, cols), f32),
            pltpu.VMEM((layers + 1, PACK, 128), f32),
            pltpu.VMEM((layers + 1, 7, PACK, 128), f32),
            dma((units + 6,)),
            dma((3,)), dma((3 * sum(PARTS),)),
            dma((1,)), dma((units,)),
            dma((1,)), dma((6,)),
            dma((1,)), dma((13,)),
            dma((layers, 2)), dma((layers, 2)),
            dma((layers + 1,)), dma((layers + 1,)),
            dma((layers,)), dma((layers, 4)),
            dma((layers,)), dma((layers, 4)),
            dma((layers,)), dma((layers, 4)),
            dma((1,)), dma((1,)),
        ],
        compiler_params=pltpu.CompilerParams(
            collective_id=0, has_side_effects=True, vmem_limit_bytes=56 * 1024 * 1024
        ),
    )(
        tokens, pre_gain, w_value, w_gate, jnp.swapaxes(all_taps, 0, 1), norm_gain, norm_shift, w_out,
        post_gain,
    )


def solution(mesh):
    nsp, ntp = mesh.shape["sp"], mesh.shape["tp"]
    body = kernel_local if nsp == 8 and ntp == 4 else local
    placed = (
        P("sp", "tp"),
        P(),
        P(None, "sp", "tp"),
        P(None, "sp", "tp"),
        P(None, None, "tp"),
        P(None, "tp"),
        P(None, "tp"),
        P(None, "tp", "sp"),
        P(None, "tp"),
    )
    return jax.shard_map(
        body, mesh=mesh, in_specs=placed, out_specs=P("sp", "tp"), check_vma=False
    )
```
